32 devices in a mesh: sp: 16 (over z, y, x), tp: 2 (over core).
Axes of the slice: x: 2, y: 2, z: 4, core: 2. Of those that a mesh axis runs over, the one named last changes fastest.
Arguments:
- tokens: bfloat16 [2048, 2048], P('sp', 'tp'), may hold values from -6 to 6
- norm_gain: float32 [2048], replicated, may hold values from 0.1 to 1.9
- w_value: bfloat16 [2048, 2048], P('sp', 'tp'), may hold values from -0.125 to 0.125
- w_gate: bfloat16 [2048, 2048], P('sp', 'tp'), may hold values from -0.125 to 0.125
- conv_taps: bfloat16 [31, 2048], P(None, 'tp'), may hold values from -1 to 1
- conv_gain: float32 [2048], P('tp'), may hold values from 0.1 to 1.9
- w_query: bfloat16 [2048, 3072], P(None, 'tp'), may hold values from -5.303301 to 5.303301
- latent_down_weight: bfloat16 [2048, 512], P('sp'), may hold values from -0.125 to 0.125
- latent_norm_gain: float32 [512], replicated, may hold values from 0.1 to 1.9
- w_rope_key: bfloat16 [2048, 64], P('sp'), may hold values from -0.125 to 0.125
- key_up_weight: bfloat16 [512, 2048], P(None, 'tp'), may hold values from -0.5 to 0.5
- value_up_weight: bfloat16 [512, 2048], P(None, 'tp'), may hold values from -0.25 to 0.25
- w_merge_conv: bfloat16 [2048, 2048], P('tp'), may hold values from -0.09375 to 0.09375
- w_merge_attn: bfloat16 [2048, 2048], P('tp'), may hold values from -0.28125 to 0.28125
Outputs:
- merged: bfloat16 [2048, 2048], P(('sp', 'tp'))
- log_sums: float32 [2048, 16], P('sp', 'tp')
The draws below stay inside these ranges and needn't reach their ends.
All inputs are finite; a program needn't handle non-finite values.
Results may differ from the reference program's by a relative error of at most 0.025.
The reference program's roundings to bfloat16 on the way count: a program that leaves them out, or rounds other values in their place, can miss the bound.
Values may be sent and summed in bfloat16 or wider, within the bound.
A program may use at most 64 MiB of HBM per device.

```python
import jax
import jax.numpy as jnp
from jax import lax

MODEL_WIDTH = 2048
CC = 2048
HEAD_TOTAL = 16
KEY_VALUE_RANK = 512
PLAIN_QK_WIDTH = 128
QK_ROPE = 64
VALUE_HEAD_WIDTH = 128
CONV_WIDTH = 31
TOKEN_TOTAL = 2048
N_TP = 2


def draw_w_query(key, part):
    values = jnp.clip(jax.random.normal(key, (MODEL_WIDTH, HEAD_TOTAL * (PLAIN_QK_WIDTH + QK_ROPE)), jnp.float32), -6.0, 6.0) * MODEL_WIDTH ** (-0.5)
    return values.astype(jnp.bfloat16)


def block_scale(rng, shape, split, smallest, largest):
    level, own = 1.0, jax.random.fold_in(rng, 6)
    for axis_at, blocks in split:
        heights = jnp.exp(jax.random.uniform(jax.random.fold_in(own, axis_at), (blocks,), jnp.float32, smallest / len(split), largest / len(split)))
        level = level * jnp.repeat(heights, shape[axis_at] // blocks).reshape([-1 if axis == axis_at else 1 for axis in range(len(shape))])
    return level


def normal_values(own_key, extent, scale, limit, pieces=(), held_as=jnp.bfloat16):
    array = scale * jax.random.normal(own_key, extent, jnp.float32)
    if pieces:
        array = array * block_scale(own_key, extent, pieces, -0.22, 0.18)
    return jnp.clip(array, -limit, limit).astype(held_as)


def setup_inputs(seed: int = 0) -> dict:
    seeds = jax.random.split(jax.random.key(seed), 15)
    return {
        "tokens": normal_values(seeds[0], (TOKEN_TOTAL, MODEL_WIDTH), 1.0, 6.0, ((0, 16), (1, 2))),
        "norm_gain": jnp.clip(1.0 + 0.18 * jax.random.normal(seeds[1], (MODEL_WIDTH,), jnp.float32), 0.1, 1.9),
        "w_value": normal_values(seeds[2], (MODEL_WIDTH, CC), MODEL_WIDTH ** -0.5, 0.125, ((0, 16), (1, 2))),
        "w_gate": normal_values(seeds[3], (MODEL_WIDTH, CC), MODEL_WIDTH ** -0.5, 0.125, ((0, 16), (1, 2))),
        "conv_taps": normal_values(seeds[4], (CONV_WIDTH, CC), CONV_WIDTH ** -0.5, 1.0, ((1, 2),)),
        "conv_gain": jnp.clip(1.0 + 0.18 * jax.random.normal(seeds[5], (CC,), jnp.float32), 0.1, 1.9),
        "w_query": draw_w_query(jax.random.fold_in(seeds[14], 71), 0),
        "latent_down_weight": normal_values(seeds[7], (MODEL_WIDTH, KEY_VALUE_RANK), MODEL_WIDTH ** -0.5, 0.125, ((0, 16),)),
        "latent_norm_gain": jnp.clip(1.0 + 0.18 * jax.random.normal(seeds[8], (KEY_VALUE_RANK,), jnp.float32), 0.1, 1.9),
        "w_rope_key": normal_values(seeds[9], (MODEL_WIDTH, QK_ROPE), MODEL_WIDTH ** -0.5, 0.125, ((0, 16),)),
        "key_up_weight": normal_values(seeds[10], (KEY_VALUE_RANK, HEAD_TOTAL * PLAIN_QK_WIDTH), PLAIN_QK_WIDTH ** -0.5, 0.5, ((1, 2),)),
        "value_up_weight": normal_values(seeds[11], (KEY_VALUE_RANK, HEAD_TOTAL * VALUE_HEAD_WIDTH), KEY_VALUE_RANK ** -0.5, 0.25, ((1, 2),)),
        "w_merge_conv": normal_values(seeds[12], (CC, MODEL_WIDTH), (CC + HEAD_TOTAL * VALUE_HEAD_WIDTH) ** -0.5, 0.09375, ((0, 2),)),
        "w_merge_attn": normal_values(seeds[13], (HEAD_TOTAL * VALUE_HEAD_WIDTH, MODEL_WIDTH), (3.0 / (CC + HEAD_TOTAL * VALUE_HEAD_WIDTH) ** 0.5), 0.28125, ((0, 2),)),
    }


epsilon = 1e-06
rope_base = 10000.0
masked_score = -1e+30

def angles_at(positions, width):
    inverse = rope_base ** (-2.0 * jnp.arange(width // 2, dtype=jnp.float32) / width)
    return positions[:, None] * inverse[None, :]

def rotate(halves, angle):
    middle = halves.shape[-1] // 2
    first, second = (halves[..., :middle], halves[..., middle:])
    cosine, sine = (jnp.cos(angle), jnp.sin(angle))
    return jnp.concatenate([first * cosine - second * sine, first * sine + second * cosine], axis=-1)

def reference(tokens, norm_gain, w_value, w_gate, conv_taps, conv_gain, w_query, latent_down_weight, latent_norm_gain, w_rope_key, key_up_weight, value_up_weight, w_merge_conv, w_merge_attn):
    features = tokens.astype(jnp.float32)
    normed = (features * lax.rsqrt(lax.optimization_barrier(jnp.mean(features * features, axis=-1, keepdims=True)) + epsilon) * norm_gain).astype(jnp.bfloat16)
    value_pre = jnp.dot(normed, w_value, preferred_element_type=jnp.float32)
    gate_pre = jnp.dot(normed, w_gate, preferred_element_type=jnp.float32)
    gated_rows = (value_pre * jax.nn.sigmoid(gate_pre)).astype(jnp.bfloat16)
    conv_reach = CONV_WIDTH - 1
    padded = jnp.concatenate([jnp.zeros((conv_reach, CC), jnp.bfloat16), gated_rows], axis=0).astype(jnp.float32)
    mixed = jnp.zeros((TOKEN_TOTAL, CC), jnp.float32)
    for tap_index in range(CONV_WIDTH):
        mixed = mixed + conv_taps[tap_index].astype(jnp.float32) * padded[tap_index:tap_index + TOKEN_TOTAL]
    channel_mean = lax.optimization_barrier(jnp.mean(mixed, axis=-1, keepdims=True))
    channel_var = lax.optimization_barrier(jnp.mean(jnp.square(mixed - channel_mean), axis=-1, keepdims=True))
    conv_out = jax.nn.silu((mixed - channel_mean) * lax.rsqrt(channel_var + epsilon) * conv_gain).astype(jnp.bfloat16)
    positions = jnp.arange(TOKEN_TOTAL, dtype=jnp.float32)
    rope_angles = angles_at(positions, QK_ROPE)
    query = jnp.dot(normed, w_query, preferred_element_type=jnp.float32).astype(jnp.bfloat16).reshape(TOKEN_TOTAL, HEAD_TOTAL, PLAIN_QK_WIDTH + QK_ROPE)
    query_rope = rotate(query[..., PLAIN_QK_WIDTH:].astype(jnp.float32), rope_angles[:, None, :]).astype(jnp.bfloat16)
    key_expanded = key_up_weight.astype(jnp.float32).reshape(KEY_VALUE_RANK, HEAD_TOTAL, PLAIN_QK_WIDTH)
    query_latent = jnp.einsum('thd,lhd->thl', query[..., :PLAIN_QK_WIDTH].astype(jnp.float32), key_expanded).astype(jnp.bfloat16)
    latent_pre = jnp.dot(normed, latent_down_weight, preferred_element_type=jnp.float32)
    latent = (latent_pre * lax.rsqrt(lax.optimization_barrier(jnp.mean(latent_pre * latent_pre, axis=-1, keepdims=True)) + epsilon) * latent_norm_gain).astype(jnp.bfloat16)
    key_rope = rotate(jnp.dot(normed, w_rope_key, preferred_element_type=jnp.float32), rope_angles).astype(jnp.bfloat16)
    score_scale = (PLAIN_QK_WIDTH + QK_ROPE) ** (-0.5)
    query_block = min(512, TOKEN_TOTAL)
    key_index = jnp.arange(TOKEN_TOTAL, dtype=jnp.int32)
    latent_wide = latent.astype(jnp.float32)
    rope_wide = key_rope.astype(jnp.float32)

    def one_block(block_start):
        block_latent = lax.dynamic_slice_in_dim(query_latent, block_start, query_block, 0).astype(jnp.float32)
        block_rope = lax.dynamic_slice_in_dim(query_rope, block_start, query_block, 0).astype(jnp.float32)
        scores = (jnp.einsum('thl,kl->thk', block_latent, latent_wide) + jnp.einsum('thr,kr->thk', block_rope, rope_wide)) * score_scale
        query_index = block_start + jnp.arange(query_block, dtype=jnp.int32)
        allowed = key_index[None, None, :] <= query_index[:, None, None]
        scores = jnp.where(allowed, scores, masked_score)
        row_max = lax.optimization_barrier(jnp.max(scores, axis=-1))
        weights = jnp.where(allowed, jnp.exp(scores - row_max[..., None]), 0.0)
        weight_sum = lax.optimization_barrier(jnp.sum(weights, axis=-1))
        weighted = jnp.einsum('thk,kl->thl', weights.astype(jnp.bfloat16).astype(jnp.float32), latent_wide)
        return ((weighted / weight_sum[..., None]).astype(jnp.bfloat16), row_max + jnp.log(weight_sum))
    block_starts = jnp.arange(TOKEN_TOTAL // query_block, dtype=jnp.int32) * query_block
    latent_result, log_sums = lax.map(one_block, block_starts)
    latent_result = latent_result.reshape(TOKEN_TOTAL, HEAD_TOTAL, KEY_VALUE_RANK)
    log_sums = log_sums.reshape(TOKEN_TOTAL, HEAD_TOTAL)
    value_expanded = value_up_weight.astype(jnp.float32).reshape(KEY_VALUE_RANK, HEAD_TOTAL, VALUE_HEAD_WIDTH)
    attention = jnp.einsum('thl,lhv->thv', latent_result.astype(jnp.float32), value_expanded).astype(jnp.bfloat16).reshape(TOKEN_TOTAL, HEAD_TOTAL * VALUE_HEAD_WIDTH)
    channel_share = CC // N_TP
    head_share = HEAD_TOTAL * VALUE_HEAD_WIDTH // N_TP
    merged = jnp.zeros((TOKEN_TOTAL, MODEL_WIDTH), jnp.float32)
    for group_index in range(N_TP):
        channel_part = conv_out[:, group_index * channel_share:(group_index + 1) * channel_share]
        head_part = attention[:, group_index * head_share:(group_index + 1) * head_share]
        partial_value = jnp.dot(channel_part, w_merge_conv[group_index * channel_share:(group_index + 1) * channel_share], preferred_element_type=jnp.float32)
        partial_value = partial_value + jnp.dot(head_part, w_merge_attn[group_index * head_share:(group_index + 1) * head_share], preferred_element_type=jnp.float32)
        merged = merged + partial_value.astype(jnp.bfloat16).astype(jnp.float32)
    return (merged.astype(jnp.bfloat16), log_sums)
```

```python
import jax
import jax.numpy as jnp
from jax import lax
from jax.experimental import pallas as pl
from jax.experimental.pallas import tpu as pltpu
from jax.sharding import PartitionSpec as P

PLAIN = 128
ROPE = 64
HEAD = PLAIN + ROPE
VALUE = 128
LANES = 128
HALO = 32

epsilon = 1e-06
rope_base = 10000.0
masked_score = -1e30
MESH = pl.DeviceIdType.MESH
ANY = pl.BlockSpec(memory_space=pl.ANY)
VMEM = pl.BlockSpec(memory_space=pltpu.VMEM)
f32, bf16 = jnp.float32, jnp.bfloat16


def each(start, stop, body):
    if stop - start <= 4:
        for k in range(start, stop):
            body(k)
    else:
        lax.fori_loop(start, stop, lambda k, c: (body(k), c)[1], 0)


def dot(a, b):
    return jnp.dot(a, b, preferred_element_type=f32)


def dot_nt(a, b):
    return lax.dot_general(a, b, (((1,), (1,)), ((), ())), preferred_element_type=f32)


class Place:
    def __init__(self, A, B1, B2, tp):
        self.A, self.B1, self.B2, self.tp = A, B1, B2, tp
        self.B = B1 * B2
        self.sp = A * self.B
        self.s = lax.axis_index("sp")
        self.t = lax.axis_index("tp")
        self.a = self.s // self.B
        self.b = lax.rem(self.s, self.B)
        self.y = self.b // B2
        self.x = lax.rem(self.b, B2)

    def at(self, a, y, x):
        return {"sp": (a * self.B1 + y) * self.B2 + x, "tp": self.t}

    def line(self, k):
        return lax.rem(self.a + k, self.A)

    def back(self, k):
        return lax.rem(self.a + self.A - k, self.A)

    def in_tp(self, k):
        return {"sp": self.s, "tp": lax.rem(self.t + k, self.tp)}


def remote(src, dst, send, recv, where):
    return pltpu.make_async_remote_copy(
        src_ref=src, dst_ref=dst, send_sem=send, recv_sem=recv, device_id=where,
        device_id_type=MESH)


class Gather:
    def __init__(self, p, ref, own, order, sems, paired=None):
        self.p, self.ref, self.own, self.order = p, ref, own, order
        self.sl, self.rl, self.sf, self.rf, self.sg, self.rg = sems
        self.paired = paired
        if isinstance(order, int):
            self.F, self.G = (p.B2, p.B1) if order else (p.B1, p.B2)
            self.cf, self.cg = (p.x, p.y) if order else (p.y, p.x)
        else:
            assert p.B1 == p.B2
            self.F = self.G = p.B1
            self.cf = p.x * order + p.y * (1 - order)
            self.cg = p.y * order + p.x * (1 - order)

    def yx(self, cf, cg):
        o = self.order
        if isinstance(o, int):
            return (cg, cf) if o else (cf, cg)
        return cg * o + cf * (1 - o), cf * o + cg * (1 - o)

    def piece(self, k, jf, jg):
        cf = lax.rem(self.cf + self.F - jf, self.F)
        cg = lax.rem(self.cg + self.G - jg, self.G)
        return self.ref(self.p.back(k), *self.yx(cf, cg))

    def line(self, k):
        p = self.p
        return remote(self.own(k), self.piece(0, 0, 0), self.sl.at[k], self.rl.at[k],
                      p.at(p.line(k), p.y, p.x))

    def source(self, k, jf):
        if isinstance(k, int) and isinstance(jf, int) and k == 0 and jf == 0:
            return self.own(0)
        return self.piece(k, jf, 0)

    def first(self, k, j):
        p = self.p
        to = self.yx(lax.rem(self.cf + j, self.F), self.cg)
        return remote(self.source(k, 0), self.piece(k, 0, 0), self.sf.at[k, j],
                      self.rf.at[k, j], p.at(p.a, *to))

    def second(self, k, jf, j):
        p = self.p
        to = self.yx(self.cf, lax.rem(self.cg + j, self.G))
        return remote(self.source(k, jf), self.piece(k, jf, 0), self.sg.at[k, jf, j],
                      self.rg.at[k, jf, j], p.at(p.a, *to))

    def spread(self, k):
        each(1, self.F, lambda j: self.first(k, j).start())
        each(1, self.G, lambda j: self.second(k, 0, j).start())

    def start_line(self):
        each(1, self.p.A, lambda k: self.line(k).start())

    def on_line(self, k):
        self.line(k).wait_recv()
        self.spread(k)

    def on_first(self, k):
        def arrived(jf):
            self.first(k, jf).wait_recv()
            each(1, self.G, lambda j: self.second(k, jf, j).start())
        each(1, self.F, arrived)

    def on_second(self, k):
        each(0, self.F, lambda jf: each(
            1, self.G, lambda j: self.second(k, jf, j).wait_recv()))
        if self.paired is not None:
            each(1, self.p.tp, lambda j: self.pair(k, j).start())

    def pair(self, k, j):
        whole, send, recv = self.paired
        here = whole(self.p.back(k))
        return remote(here, here, send.at[k, j], recv.at[k, j], self.p.in_tp(j))

    def on_pair(self, k):
        if self.paired is not None:
            each(1, self.p.tp, lambda j: self.pair(k, j).wait_recv())

    def drain(self):
        p = self.p
        each(1, p.A, lambda k: self.line(k).wait_send())

        def out(k):
            each(1, self.F, lambda j: self.first(k, j).wait_send())
            each(0, self.F, lambda jf: each(
                1, self.G, lambda j: self.second(k, jf, j).wait_send()))
            if self.paired is not None:
                each(1, p.tp, lambda j: self.pair(k, j).wait_send())
        each(0, p.A, out)


def swap_halves(v, lane):
    low = lax.rem(lane, ROPE) < ROPE // 2
    return jnp.where(low, pltpu.roll(v, LANES - ROPE // 2, 1), pltpu.roll(v, ROPE // 2, 1))


def kernel(A, B1, B2, tp, dtp,
           tok, wv, wg, wq, ld, wr, kup, vup, wmc, wma,
           gain, lgain, cgain, taps, cosine, sine,
           hold, row_max, row_sum,
           xin, xb, vb, gb, db, kb, dl, dr, wqb, kupb, vupb, wmcb, wmab, qs, acc, mx, sm,
           att, pacc, gated, cb, mixed, st, pb,
           lsem, tsend, trecv, zsend, zrecv, psend, precv,
           dls, dlr, dfs, dfr, dgs, dgr, dps, dpr,
           kls, klr, kfs, kfr, kgs, kgr, kps, kpr,
           vls, vlr, vfs, vfr, vgs, vgr,
           gls, glr, gfs, gfr, ggs, ggr,
           wsend, wrecv, hsend, hrecv, ssend, srecv, msend, mrecv):
    p = Place(A, B1, B2, tp)
    B, sp, a, s, t = p.B, p.sp, p.a, p.s, p.t
    R, F = tok.shape
    D = wq.shape[0]
    L = ld.shape[1]
    E = L + ROPE
    C = wv.shape[1]
    W = C // A
    heads = wq.shape[1] // HEAD
    Rk = R // tp
    mine = pl.ds(pl.multiple_of(t * F, F), F)
    columns = lambda k: pl.ds(pl.multiple_of(p.line(k) * W, W), W)

    locals_ = []

    def load(src, dst):
        c = pltpu.make_async_copy(src, dst, lsem.at[len(locals_)])
        locals_.append(c)
        c.start()
        return c

    drows = ld.shape[0] // dtp
    td = t if dtp > 1 else 0
    dpart = pl.ds(pl.multiple_of(td * drows, drows), drows)
    c_tok = load(tok, xin.at[:, mine])
    c_ld = load(ld.at[dpart], dl)
    c_wr = load(wr.at[dpart], dr)
    c_v = load(wv.at[:, columns(0)], vb.at[a, p.y, p.x])
    c_g = load(wg.at[:, columns(0)], gb.at[a, p.y, p.x])
    step = 2 * HEAD
    c_wq = [load(wq.at[:, pl.ds(i * step, step)], wqb.at[:, pl.ds(i * step, step)])
            for i in range(heads // 2)]
    c_kup = load(kup, kupb)
    c_vup = load(vup, vupb)
    c_wma = load(wma, wmab)
    c_wmc = load(wmc, wmcb)

    barrier = pltpu.get_barrier_semaphore()
    lax.fori_loop(1, sp, lambda k, c: (pl.semaphore_signal(
        barrier, inc=1, device_id={"sp": lax.rem(s + k, sp), "tp": t},
        device_id_type=MESH), c)[1], 0)
    lax.fori_loop(1, tp, lambda k, c: (pl.semaphore_signal(
        barrier, inc=1, device_id=p.in_tp(k), device_id_type=MESH), c)[1], 0)
    pl.semaphore_wait(barrier, sp - 1 + tp - 1)

    by_core = 1 - lax.rem(t, 2) if B1 == B2 else 1
    down = Gather(p, lambda i, y, x: db.at[i, y, x, td],
                  lambda k: db.at[a, p.y, p.x, td], by_core,
                  (dls, dlr, dfs, dfr, dgs, dgr),
                  (lambda i: db.at[i, :, :, td], dps, dpr) if dtp > 1 else None)
    keys = Gather(p, lambda i, y, x: kb.at[i, y, x, t],
                  lambda k: kb.at[a, p.y, p.x, t], by_core,
                  (kls, klr, kfs, kfr, kgs, kgr),
                  (lambda i: kb.at[i, :, :, t], kps, kpr))
    value = Gather(p, lambda i, y, x: vb.at[i, y, x],
                   lambda k: wv.at[:, columns(k)], 1, (vls, vlr, vfs, vfr, vgs, vgr))
    gate = Gather(p, lambda i, y, x: gb.at[i, y, x],
                  lambda k: wg.at[:, columns(k)], 0, (gls, glr, gfs, gfr, ggs, ggr))

    tok_pair = lambda k: remote(tok, xin.at[:, mine], tsend.at[k], trecv.at[k], p.in_tp(k))
    each(1, tp, lambda k: tok_pair(k).start())
    c_ld.wait()
    c_wr.wait()
    db[a, p.y, p.x, td, :, :L] = dl[...]
    db[a, p.y, p.x, td, :, L:] = dr[...]
    down.start_line()
    down.spread(0)
    value.spread(0)
    gate.spread(0)
    value.start_line()
    gate.start_line()

    c_tok.wait()
    each(1, tp, lambda k: tok_pair(k).wait_recv())
    NR = 32 if R % 32 == 0 else R

    def norm(i, c):
        rows = pl.ds(pl.multiple_of(i * NR, NR), NR)
        v = xin[rows].astype(f32)
        scale = lax.rsqrt(jnp.mean(v * v, axis=-1, keepdims=True) + epsilon)
        xb[a, rows] = (v * scale * gain[...]).astype(bf16)
        return c
    lax.fori_loop(0, R // NR, norm, 0)

    def hop(way, j):
        i = jnp.clip(a + (-j if way == 0 else j), 0, A - 1)
        to = jnp.clip(a + (1 if way == 0 else -1), 0, A - 1)
        return remote(xb.at[i, :, mine], xb.at[i, :, mine], zsend.at[way, j],
                      zrecv.at[way, j], p.at(to, p.y, p.x))

    def across(way, j, k):
        i = jnp.clip(a + (-j if way == 0 else j), 0, A - 1)
        return remote(xb.at[i, :, mine], xb.at[i, :, mine], psend.at[way, j, k],
                      precv.at[way, j, k], p.in_tp(k))

    def has(way, j):
        return a - j >= 0 if way == 0 else a + j < A

    def onward(way):
        return a + 1 < A if way == 0 else a >= 1

    def start_hop(way, j):
        if j < A - 1:
            pl.when(jnp.logical_and(has(way, j), onward(way)))(lambda: hop(way, j).start())

    def token_step(j):
        for way in (0, 1):
            def got(way=way):
                hop(way, j - 1).wait_recv()
                each(1, tp, lambda k: across(way, j, k).start())
            pl.when(has(way, j))(got)
            start_hop(way, j)

    start_hop(0, 0)
    start_hop(1, 0)
    for k in range(1, A):
        down.on_line(k)

    lane = lax.broadcasted_iota(jnp.int32, (R, LANES), 1)
    c_kup.wait()

    def query(i):
        c_wq[i].wait()
        q = dot(xb[a], wqb[:, i * step:(i + 1) * step]).astype(bf16).astype(f32)
        q0, q1, q2 = q[:, :LANES], q[:, LANES:2 * LANES], q[:, 2 * LANES:]
        left = lane < ROPE
        second = jnp.where(left, pltpu.roll(q1, ROPE, 1), pltpu.roll(q2, ROPE, 1))
        ropes = jnp.where(left, q1, q2)
        turned = ropes * cosine[...] + swap_halves(ropes, lane) * sine[...]
        for h, plain, rope in ((0, q0, turned), (1, second, pltpu.roll(turned, ROPE, 1))):
            at = 2 * i + h
            up = kupb[:, at * PLAIN:(at + 1) * PLAIN]
            rows = pl.ds(at * R, R)
            qs[rows, :L] = dot_nt(plain.astype(bf16), up).astype(bf16)
            qs[rows, L:] = rope[:, :ROPE].astype(bf16)

    query(0)
    for k in range(A):
        down.on_first(k)
    for k in range(1, A):
        value.on_line(k)
        gate.on_line(k)
    for k in range(A):
        down.on_second(k)
    for i in range(1, heads // 2):
        query(i)
    for k in range(A):
        down.on_pair(k)

    own = xb[a, pl.ds(pl.multiple_of(t * Rk, Rk), Rk)]
    span = D // A
    pre = jnp.zeros((Rk, E), f32)
    for i in range(A):
        pre = pre + dot(own[:, i * span:(i + 1) * span], db[i].reshape(span, E))
    lat = pre[:, :L]
    lat = lat * lax.rsqrt(jnp.mean(lat * lat, axis=-1, keepdims=True) + epsilon) * lgain[...]
    rope = jnp.concatenate([pre[:, L:], pre[:, L:]], axis=1)
    krows = pl.ds(pl.multiple_of(t * Rk, Rk), Rk)
    rope = rope * cosine[krows] + swap_halves(rope, lane[:Rk]) * sine[krows]
    kb[a, p.y, p.x, t, :, :L] = lat.astype(bf16)
    kb[a, p.y, p.x, t, :, L:] = rope[:, :ROPE].astype(bf16)
    for k in range(A):
        value.on_first(k)
        gate.on_first(k)
    keys.start_line()
    keys.spread(0)
    if A > 1:
        token_step(1)
    for k in range(1, A):
        keys.on_line(k)
    for j in range(2, A - 1):
        token_step(j)
    for k in range(A):
        keys.on_first(k)
    for k in range(A):
        keys.on_second(k)

    mx[...] = jnp.full(mx.shape, masked_score, f32)
    sm[...] = jnp.zeros(sm.shape, f32)
    acc[...] = jnp.zeros(acc.shape, f32)
    scale = HEAD ** (-0.5)
    per = 1
    while per < B2 and (per * 2) * R <= 512 and B2 % (per * 2) == 0:
        per *= 2
    tall = 1
    if per == B2:
        while tall < B1 and (tall * 2) * per * R <= 512 and B1 % (tall * 2) == 0:
            tall *= 2
    KS = tall * per * R
    QR = 2 * R

    def attend(i, k0, kk):
        rows = pl.ds(pl.multiple_of(i * QR, QR), QR)
        sc = dot_nt(qs[rows], kk) * scale
        at = lax.broadcasted_iota(jnp.int32, (QR, KS), 0)
        kp = lax.broadcasted_iota(jnp.int32, (QR, KS), 1)
        allowed = k0 + kp <= s * R + lax.rem(at, R)
        sc = jnp.where(allowed, sc, masked_score)
        old = mx[rows, :1]
        new = jnp.maximum(old, jnp.max(sc, axis=1, keepdims=True))
        w = jnp.where(allowed, jnp.exp(sc - new), 0.0)
        fade = jnp.exp(old - new)
        sm[rows] = jnp.broadcast_to(
            fade * sm[rows, :1] + jnp.sum(w, axis=1, keepdims=True), (QR, LANES))
        mx[rows] = jnp.broadcast_to(new, (QR, LANES))
        acc[rows] = fade * acc[rows] + dot(w.astype(bf16), kk[:, :L])

    def chunk(k):
        keys.on_pair(k)

        def go():
            c = p.back(k)

            def sub(n, carry):
                y0 = n // (B2 // per) * tall
                x0 = lax.rem(n, B2 // per) * per
                kk = kb[c, pl.ds(y0, tall), pl.ds(x0, per)].reshape(KS, E)
                k0 = (c * B + y0 * B2 + x0) * R
                lax.fori_loop(0, heads // 2, lambda i, q: (attend(i, k0, kk), q)[1], 0)
                return carry
            if B * R == KS:
                sub(0, 0)
            else:
                lax.fori_loop(0, B * R // KS, sub, 0)
        pl.when(k <= a)(go)

    for k in range(A):
        chunk(k)

    c_vup.wait()
    c_wma.wait()
    hl = lax.broadcasted_iota(jnp.int32, (R, heads), 1)
    top = jnp.zeros((R, heads), f32)
    total = jnp.zeros((R, heads), f32)
    for h in range(heads):
        rows = pl.ds(h * R, R)
        out = (acc[rows] / sm[rows, :1]).astype(bf16)
        att[:, h * VALUE:(h + 1) * VALUE] = dot(
            out, vupb[:, h * VALUE:(h + 1) * VALUE]).astype(bf16)
        top = jnp.where(hl == h, mx[rows, :1], top)
        total = jnp.where(hl == h, sm[rows, :1], total)
    row_max[...] = top
    row_sum[...] = total
    NT = 512
    nt = D // NT

    def attn_merge(n, c):
        cols = pl.ds(pl.multiple_of(n * NT, NT), NT)
        pacc[:, cols] = dot(att[...], wmab[:, cols])
        return c
    lax.fori_loop(0, nt, attn_merge, 0)

    if A > 2:
        pass
    if A > 1:
        j = A - 1
        if j > 1:
            token_step(j)
    for k in range(A):
        value.on_second(k)
        gate.on_second(k)
    c_v.wait()
    c_g.wait()
    for way in (0, 1):
        for j in range(1, A):
            pl.when(has(way, j))(lambda way=way, j=j: each(
                1, tp, lambda k: across(way, j, k).wait_recv()))

    swap = lambda k: remote(
        gated.at[p.line(k)], cb.at[a, pl.ds(HALO, R)], wsend.at[k], wrecv.at[k],
        p.at(p.line(k), p.y, p.x))

    def after(i):
        return i * B + p.b + 1

    def halo(k):
        i = p.line(k)
        to = jnp.minimum(after(i), sp - 1)
        return remote(gated.at[i, pl.ds(R - HALO, HALO)], cb.at[a, pl.ds(0, HALO)],
                      hsend.at[k], hrecv.at[k], {"sp": to, "tp": t})

    vw = vb[...].reshape(D, W)
    gw = gb[...].reshape(D, W)
    for k in list(range(1, A)) + [0]:
        i = p.line(k)
        rows = xb[i]
        v = dot(rows, vw)
        g = dot(rows, gw)
        gated[i] = (v / (1.0 + jnp.exp(-g))).astype(bf16)
        if k == 0:
            cb[a, HALO:] = gated[a]
        else:
            swap(k).start()
        pl.when(after(i) < sp)(lambda k=k: halo(k).start())

    pl.when(s == 0)(lambda: cb.__setitem__(
        (slice(None), slice(0, HALO)), jnp.zeros((A, HALO, W), bf16)))

    def halos():
        for k in range(A):
            halo(k).wait_recv()
    pl.when(s > 0)(halos)
    reach = taps.shape[0] - 1
    lead = HALO - reach
    whole = R + HALO
    wb = W // LANES

    def convolve(n, c):
        i = n // wb
        cols = pl.ds(pl.multiple_of(lax.rem(n, wb) * LANES, LANES), LANES)
        full = pl.ds(pl.multiple_of(n * LANES, LANES), LANES)
        xf = cb[i, :, cols].astype(f32)
        tw = taps[:, full].astype(f32)
        out = jnp.zeros((R, LANES), f32)
        for r in range(8):
            xr = xf if r == 0 else pltpu.roll(xf, whole - r, 0)
            for m in range(HALO // 8 + 1):
                j = 8 * m + r - lead
                if 0 <= j <= reach:
                    out = out + tw[j:j + 1] * xr[8 * m:8 * m + R]
        mixed[:, full] = out
        return c

    for k in range(1, A):
        swap(k).wait_recv()
    lax.fori_loop(0, A * wb, convolve, 0)
    all_mixed = mixed[...]
    one = jnp.sum(all_mixed, axis=1, keepdims=True)
    two = jnp.sum(all_mixed * all_mixed, axis=1, keepdims=True)
    st[t] = jnp.where(lane == 0, one, jnp.where(lane == 1, two, 0.0))
    stats = lambda k: remote(st.at[t], st.at[t], ssend.at[k], srecv.at[k], p.in_tp(k))
    each(1, tp, lambda k: stats(k).start())
    each(1, tp, lambda k: stats(k).wait_recv())
    both = jnp.sum(st[...], axis=0)
    mean = both[:, :1] / (C * tp)
    var = both[:, 1:2] / (C * tp) - mean * mean
    z = (mixed[...] - mean) * lax.rsqrt(var + epsilon) * cgain[...]
    out = (z / (1.0 + jnp.exp(-z))).astype(bf16)

    c_wmc.wait()
    share = lambda n, k: remote(
        pb.at[lax.rem(t + k, tp), :, pl.ds(n * NT, NT)], hold.at[t, :, pl.ds(n * NT, NT)],
        msend.at[n, k], mrecv.at[n, k], p.in_tp(k))
    for n in range(nt):
        cols = slice(n * NT, (n + 1) * NT)
        part = (dot(out, wmcb[:, cols]) + pacc[:, cols]).astype(bf16)
        for j in range(tp):
            pb[j, :, cols] = part[j * Rk:(j + 1) * Rk]
        each(1, tp, lambda k: share(n, k).start())
    keep = pltpu.make_async_copy(pb.at[t], hold.at[t], lsem.at[len(locals_)])
    keep.start()

    each(1, tp, lambda k: tok_pair(k).wait_send())
    for g in (down, keys, value, gate):
        g.drain()
    for way in (0, 1):
        for j in range(A - 1):
            pl.when(jnp.logical_and(has(way, j), onward(way)))(
                lambda way=way, j=j: hop(way, j).wait_send())
        for j in range(1, A):
            pl.when(has(way, j))(lambda way=way, j=j: each(
                1, tp, lambda k: across(way, j, k).wait_send()))
    for k in range(A):
        if k:
            swap(k).wait_send()
        pl.when(after(p.line(k)) < sp)(lambda k=k: halo(k).wait_send())
    each(1, tp, lambda k: stats(k).wait_send())
    for n in range(nt):
        each(1, tp, lambda k: share(n, k).wait())
    keep.wait()


def rope_tables(first_row, count):
    inverse = rope_base ** (-2.0 * jnp.arange(ROPE // 2, dtype=f32) / ROPE)
    inverse = jnp.concatenate([inverse] * (LANES * 2 // ROPE))
    sign = jnp.where(jnp.arange(LANES) % ROPE < ROPE // 2, -1.0, 1.0).astype(f32)
    position = (first_row + jnp.arange(count, dtype=jnp.int32)).astype(f32)
    angle = position[:, None] * inverse[None, :]
    return jnp.cos(angle), jnp.sin(angle) * sign[None, :]


def local(tokens, norm_gain, w_value, w_gate, conv_taps, conv_gain, w_query,
          latent_down_weight, latent_norm_gain, w_rope_key, key_up_weight,
          value_up_weight, w_merge_conv, w_merge_attn):
    R, F = tokens.shape
    sp, tp = lax.axis_size("sp"), lax.axis_size("tp")
    C = w_value.shape[1]
    A = 1
    while A < 4 and sp % (2 * A) == 0 and C % (2 * A * LANES) == 0:
        A *= 2
    B = sp // A
    B2 = 1
    while B2 * B2 < B and B % (2 * B2) == 0:
        B2 *= 2
    B1 = B // B2
    D = w_query.shape[0]
    L = latent_down_weight.shape[1]
    E = L + ROPE
    W = C // A
    Kr = w_value.shape[0]
    heads = w_query.shape[1] // HEAD
    Rk = R // tp
    dtp = tp if Kr % (16 * tp) == 0 else 1
    NT = D // 512
    cosine, sine = rope_tables(lax.axis_index("sp") * R, R)
    S = pltpu.SemaphoreType.DMA
    V = pltpu.VMEM
    two = lambda *n: [S(n), S(n)]
    most = max(B1, B2)
    gather = lambda: two(A) + two(A, most) + two(A, most, most)
    sds = jax.ShapeDtypeStruct
    row = lambda v: v.reshape(1, -1)
    hold, row_max, row_sum = pl.pallas_call(
        lambda *refs: kernel(A, B1, B2, tp, dtp, *refs),
        out_shape=(sds((tp, Rk, D), bf16), sds((R, heads), f32), sds((R, heads), f32)),
        in_specs=[ANY] * 10 + [VMEM] * 6,
        out_specs=(ANY, VMEM, VMEM),
        scratch_shapes=[
            V((R, D), bf16), V((A, R, D), bf16),
            V((A, B1, B2, Kr, W), bf16), V((A, B1, B2, Kr, W), bf16),
            V((A, B1, B2, dtp, Kr // dtp, E), bf16), V((A, B1, B2, tp, Rk, E), bf16),
            V((Kr // dtp, L), bf16), V((Kr // dtp, ROPE), bf16),
            V(w_query.shape, bf16), V(key_up_weight.shape, bf16),
            V(value_up_weight.shape, bf16), V(w_merge_conv.shape, bf16),
            V(w_merge_attn.shape, bf16),
            V((heads * R, E), bf16), V((heads * R, L), f32),
            V((heads * R, LANES), f32), V((heads * R, LANES), f32),
            V((R, heads * VALUE), bf16), V((R, D), f32),
            V((A, R, W), bf16), V((A, R + HALO, W), bf16), V((R, C), f32),
            V((tp, R, LANES), f32), V((tp, Rk, D), bf16),
            S((10 + heads // 2,)), *two(tp), *two(2, A), *two(2, A, tp),
            *gather(), *two(A, tp), *gather(), *two(A, tp), *gather(), *gather(),
            *two(A), *two(A), *two(tp), *two(NT, tp),
        ],
        compiler_params=pltpu.CompilerParams(
            collective_id=0, has_side_effects=True, vmem_limit_bytes=60 * 2**20),
        name="layer",
    )(tokens, w_value, w_gate, w_query, latent_down_weight, w_rope_key, key_up_weight,
      value_up_weight, w_merge_conv, w_merge_attn, row(norm_gain), row(latent_norm_gain),
      row(conv_gain), conv_taps, cosine, sine)
    merged = jnp.sum(hold.astype(f32), axis=0).astype(bf16)
    return merged, row_max + jnp.log(row_sum)


def solution(mesh):
    return jax.shard_map(
        local,
        mesh=mesh,
        in_specs=(
            P("sp", "tp"), P(), P("sp", "tp"), P("sp", "tp"), P(None, "tp"), P("tp"),
            P(None, "tp"), P("sp", None), P(), P("sp", None), P(None, "tp"),
            P(None, "tp"), P("tp", None), P("tp", None),
        ),
        out_specs=(P(("sp", "tp"), None), P("sp", "tp")),
        check_vma=False,
    )
```

```python
import jax
import jax.numpy as jnp
import numpy as np
from jax import lax
from jax.experimental import pallas as pl
from jax.experimental.pallas import tpu as pltpu
from jax.sharding import PartitionSpec as P

PLAIN = 128
ROPE = 64
HEAD = PLAIN + ROPE
VALUE = 128
LANES = 128
HALO = 32

epsilon = 1e-06
rope_base = 10000.0
masked_score = -1e30
MESH = pl.DeviceIdType.MESH
ANY = pl.BlockSpec(memory_space=pl.ANY)
VMEM = pl.BlockSpec(memory_space=pltpu.VMEM)
f32, bf16 = jnp.float32, jnp.bfloat16


def each(start, stop, body):
    if stop - start <= 4:
        for k in range(start, stop):
            body(k)
    else:
        lax.fori_loop(start, stop, lambda k, c: (body(k), c)[1], 0)


def dot(a, b):
    return jnp.dot(a, b, preferred_element_type=f32)


def dot_nt(a, b):
    return lax.dot_general(a, b, (((1,), (1,)), ((), ())), preferred_element_type=f32)


ROWS = 256
UNROLL = 4


ORDER = (
    "down_own", "down_line.2", "rope_own", "down_line.1", "gate_spread", "value_spread",
    "tok_start", "down_line.3", "value_2.0", "down_2.0", "down_1.2", "value_line.2",
    "down_2.2", "gate_line.2", "down_1.3", "gate_2.0", "value_line.3", "gate_line.1",
    "down_3.0", "down_1.1", "norm", "tok_0", "value_line.1", "down_2.3", "down_3.3",
    "value_1.2", "gate_line.3", "down_4.0", "down_2.1", "down_3.2", "gate_1.2", "query_0",
    "query_1", "down_4.3", "down_3.1", "value_1.3", "gate_1.1", "gate_2.2", "tok_1",
    "down_4.2", "down_4.1", "keys_own", "keys_line.3", "keys_spread", "keys_line.2",
    "query_4", "keys_2.0", "value_2.3", "attend_init", "query_3", "value_1.1", "query_2",
    "gate_2.1", "gate_1.3", "keys_3.0", "value_2.2", "keys_line.1", "keys_1.3", "gate_3.1",
    "tok_2", "keys_1.1", "value_3.2", "value_3.0", "keys_2.3", "gate_3.0", "value_2.1",
    "gate_2.3", "gate_3.2", "keys_2.1", "keys_4.0", "keys_1.2", "attend_0", "keys_2.2",
    "gate_3.3", "keys_3.3", "tok_3", "value_3.1", "value_3.3", "wready", "keys_3.1",
    "gated_1", "gated_2", "gated_0", "keys_3.2", "keys_4.1", "keys_4.3", "attend_1",
    "keys_4.2", "gated_3", "attend_3", "attend_2", "conv", "attend_out", "finish",
)


class Place:
    def __init__(self, A, B1, B2, tp):
        self.A, self.B1, self.B2, self.tp = A, B1, B2, tp
        self.B = B1 * B2
        self.sp = A * self.B
        self.s = lax.axis_index("sp")
        self.t = lax.axis_index("tp")
        self.a = self.s // self.B
        self.b = lax.rem(self.s, self.B)
        self.y = self.b // B2
        self.x = lax.rem(self.b, B2)

    def at(self, a, y, x):
        return {"sp": (a * self.B1 + y) * self.B2 + x, "tp": self.t}

    def line(self, k):
        return lax.rem(self.a + k, self.A)

    def back(self, k):
        return lax.rem(self.a + self.A - k, self.A)

    def in_tp(self, k):
        return {"sp": self.s, "tp": lax.rem(self.t + k, self.tp)}


def remote(src, dst, send, recv, where):
    return pltpu.make_async_remote_copy(
        src_ref=src, dst_ref=dst, send_sem=send, recv_sem=recv, device_id=where,
        device_id_type=MESH)


class Gather:
    def __init__(self, p, ref, own, order, sems, paired=None):
        self.p, self.ref, self.own, self.order = p, ref, own, order
        self.sl, self.rl, self.sf, self.rf, self.sg, self.rg = sems
        self.paired = paired
        if isinstance(order, int):
            self.F, self.G = (p.B2, p.B1) if order else (p.B1, p.B2)
            self.cf, self.cg = (p.x, p.y) if order else (p.y, p.x)
        else:
            assert p.B1 == p.B2
            self.F = self.G = p.B1
            self.cf = p.x * order + p.y * (1 - order)
            self.cg = p.y * order + p.x * (1 - order)

    def yx(self, cf, cg):
        o = self.order
        if isinstance(o, int):
            return (cg, cf) if o else (cf, cg)
        return cg * o + cf * (1 - o), cf * o + cg * (1 - o)

    def piece(self, k, jf, jg):
        cf = lax.rem(self.cf + self.F - jf, self.F)
        cg = lax.rem(self.cg + self.G - jg, self.G)
        return self.ref(self.p.back(k), *self.yx(cf, cg))

    def line(self, k):
        p = self.p
        return remote(self.own(k), self.piece(0, 0, 0), self.sl.at[k - 1], self.rl.at[k - 1],
                      p.at(p.line(k), p.y, p.x))

    def source(self, k, jf):
        if isinstance(k, int) and isinstance(jf, int) and k == 0 and jf == 0:
            return self.own(0)
        return self.piece(k, jf, 0)

    def first(self, k, j):
        p = self.p
        to = self.yx(lax.rem(self.cf + j, self.F), self.cg)
        return remote(self.source(k, 0), self.piece(k, 0, 0), self.sf.at[k, j - 1],
                      self.rf.at[k, j - 1], p.at(p.a, *to))

    def second(self, k, jf, j):
        p = self.p
        to = self.yx(self.cf, lax.rem(self.cg + j, self.G))
        return remote(self.source(k, jf), self.piece(k, jf, 0), self.sg.at[k, jf, j - 1],
                      self.rg.at[k, jf, j - 1], p.at(p.a, *to))

    def spread(self, k):
        each(1, self.F, lambda j: self.first(k, j).start())
        each(1, self.G, lambda j: self.second(k, 0, j).start())

    def on_line(self, k):
        self.line(k).wait_recv()
        self.spread(k)

    def on_first(self, k):
        def arrived(jf):
            self.first(k, jf).wait_recv()
            each(1, self.G, lambda j: self.second(k, jf, j).start())
        each(1, self.F, arrived)

    def on_second(self, k):
        each(0, self.F, lambda jf: each(
            1, self.G, lambda j: self.second(k, jf, j).wait_recv()))
        if self.paired is not None:
            each(1, self.p.tp, lambda j: self.pair(k, j).start())

    def pair(self, k, j):
        whole, send, recv = self.paired
        here = whole(self.p.back(k))
        return remote(here, here, send.at[k, j - 1], recv.at[k, j - 1], self.p.in_tp(j))

    def on_pair(self, k):
        if self.paired is not None:
            each(1, self.p.tp, lambda j: self.pair(k, j).wait_recv())

    def drain(self):
        p = self.p
        each(1, p.A, lambda k: self.line(k).wait_send())

        def out(k):
            each(1, self.F, lambda j: self.first(k, j).wait_send())
            each(0, self.F, lambda jf: each(
                1, self.G, lambda j: self.second(k, jf, j).wait_send()))
            if self.paired is not None:
                each(1, p.tp, lambda j: self.pair(k, j).wait_send())
        each(0, p.A, out)


def swap_halves(v, lane):
    low = lax.rem(lane, ROPE) < ROPE // 2
    return jnp.where(low, pltpu.roll(v, LANES - ROPE // 2, 1), pltpu.roll(v, ROPE // 2, 1))


def kernel(A, B1, B2, tp, dtp,
           tok, wv, wg, wq, ld, wr, kup, vup, wmc, wma,
           gain, lgain, cgain, taps, near, far,
           hold, logs,
           cosine, sine, xin, xb, vb, gb, db, kb, dl, dr, drt, wqb, kupb, vupb, wmcb, wmab, qs, acc, mx, sm,
           att, pacc, gated, cb, mixed, st, pb,
           lsem, tsend, trecv, zsend, zrecv, psend, precv,
           dls, dlr, dfs, dfr, dgs, dgr, dps, dpr,
           kls, klr, kfs, kfr, kgs, kgr, kps, kpr,
           vls, vlr, vfs, vfr, vgs, vgr,
           gls, glr, gfs, gfr, ggs, ggr,
           wsend, wrecv, hsend, hrecv, ssend, srecv, msend, mrecv):
    p = Place(A, B1, B2, tp)
    B, sp, a, s, t = p.B, p.sp, p.a, p.s, p.t
    R, F = tok.shape
    D = wq.shape[0]
    L = ld.shape[1]
    E = L + ROPE
    C = wv.shape[1]
    W = C // A
    heads = wq.shape[1] // HEAD
    Rk = R // tp
    mine = pl.ds(pl.multiple_of(t * F, F), F)
    columns = lambda k: pl.ds(pl.multiple_of(p.line(k) * W, W), W)

    locals_ = []

    def load(src, dst):
        c = pltpu.make_async_copy(src, dst, lsem.at[len(locals_)])
        locals_.append(c)
        c.start()
        return c

    drows = ld.shape[0] // dtp
    td = t if dtp > 1 else 0
    dpart = pl.ds(pl.multiple_of(td * drows, drows), drows)
    c_tok = load(tok, xin.at[:, mine])
    c_ld = load(ld.at[dpart], dl)
    c_wr = load(wr, dr)
    c_v = load(wv.at[:, columns(0)], vb.at[a, p.y, p.x])
    c_g = load(wg.at[:, columns(0)], gb.at[a, p.y, p.x])
    step = 2 * HEAD
    c_wq = [load(wq.at[:, pl.ds(i * step, step)], wqb.at[:, pl.ds(i * step, step)])
            for i in range(heads // 2)]
    c_kup = load(kup, kupb)
    c_vup = load(vup, vupb)
    c_wma = load(wma, wmab)
    c_wmc = load(wmc, wmcb)

    barrier = pltpu.get_barrier_semaphore()
    lax.fori_loop(1, sp, lambda k, c: (pl.semaphore_signal(
        barrier, inc=1, device_id={"sp": lax.rem(s + k, sp), "tp": t},
        device_id_type=MESH), c)[1], 0)
    lax.fori_loop(1, tp, lambda k, c: (pl.semaphore_signal(
        barrier, inc=1, device_id=p.in_tp(k), device_id_type=MESH), c)[1], 0)
    pl.semaphore_wait(barrier, sp - 1 + tp - 1)

    by_core = 1 - lax.rem(t, 2) if B1 == B2 else 1
    down = Gather(p, lambda i, y, x: db.at[i, y, x, td],
                  lambda k: db.at[a, p.y, p.x, td], by_core,
                  (dls, dlr, dfs, dfr, dgs, dgr),
                  (lambda i: db.at[i, :, :, td], dps, dpr) if dtp > 1 else None)
    keys = Gather(p, lambda i, y, x: kb.at[i, y, x, t],
                  lambda k: kb.at[a, p.y, p.x, t], by_core,
                  (kls, klr, kfs, kfr, kgs, kgr),
                  (lambda i: kb.at[i, :, :, t], kps, kpr))
    value = Gather(p, lambda i, y, x: vb.at[i, y, x],
                   lambda k: wv.at[:, columns(k)], 1, (vls, vlr, vfs, vfr, vgs, vgr))
    gate = Gather(p, lambda i, y, x: gb.at[i, y, x],
                  lambda k: wg.at[:, columns(k)], 0, (gls, glr, gfs, gfr, ggs, ggr))

    lane = lax.broadcasted_iota(jnp.int32, (R, LANES), 1)
    tok_pair = lambda k: remote(tok, xin.at[:, mine], tsend.at[k - 1], trecv.at[k - 1], p.in_tp(k))
    steps = {}

    def named(f):
        steps[f.__name__] = f
        return f

    @named
    def tok_start():
        each(1, tp, lambda k: tok_pair(k).start())

    @named
    def down_own():
        c_ld.wait()
        c_wr.wait()
        drt[...] = dr[...].astype(f32).T
        db[a, p.y, p.x, td, :, :L] = dl[...]
        db[a, p.y, p.x, td, :, L:] = drt[dpart].astype(bf16)
        down.spread(0)

    for name, g in (("down", down), ("keys", keys), ("value", value), ("gate", gate)):
        steps[name + "_spread"] = lambda g=g: g.spread(0)
        for k in range(A):
            if k:
                steps[f"{name}_line.{k}"] = lambda g=g, k=k: g.line(k).start()
                steps[f"{name}_1.{k}"] = lambda g=g, k=k: g.on_line(k)
            steps[f"{name}_2.{k}"] = lambda g=g, k=k: g.on_first(k)
            steps[f"{name}_3.{k}"] = lambda g=g, k=k: g.on_second(k)
            steps[f"{name}_4.{k}"] = lambda g=g, k=k: g.on_pair(k)

    NR = 32 if R % 32 == 0 else R

    @named
    def norm():
        c_tok.wait()
        each(1, tp, lambda k: tok_pair(k).wait_recv())

        def rows_norm(i, c):
            rows = pl.ds(pl.multiple_of(i * NR, NR), NR)
            v = xin[rows].astype(f32)
            scale = lax.rsqrt(jnp.mean(v * v, axis=-1, keepdims=True) + epsilon)
            xb[a, rows] = (v * scale * gain[...]).astype(bf16)
            return c
        lax.fori_loop(0, R // NR, rows_norm, 0)

    @named
    def rope_own():
        c0, s0 = far[0, pl.ds(s, 1)], far[1, pl.ds(s, 1)]
        cosine[...] = near[0] * c0 - near[1] * s0
        sine[...] = near[1] * c0 + near[0] * s0

    def hop(way, j):
        i = jnp.clip(a + (-j if way == 0 else j), 0, A - 1)
        to = jnp.clip(a + (1 if way == 0 else -1), 0, A - 1)
        return remote(xb.at[i, :, mine], xb.at[i, :, mine], zsend.at[way, j],
                      zrecv.at[way, j], p.at(to, p.y, p.x))

    def across(way, j, k):
        i = jnp.clip(a + (2 * way - 1) * j, 0, A - 1)
        return remote(xb.at[i, :, mine], xb.at[i, :, mine], psend.at[way, j - 1, k - 1],
                      precv.at[way, j - 1, k - 1], p.in_tp(k))

    def has(way, j):
        return a - j >= 0 if way == 0 else a + j < A

    def onward(way):
        return a + 1 < A if way == 0 else a >= 1

    def start_hop(way, j):
        if j < A - 1:
            pl.when(jnp.logical_and(has(way, j), onward(way)))(lambda: hop(way, j).start())

    def token_step(j):
        for way in (0, 1):
            def got(way=way):
                hop(way, j - 1).wait_recv()
                each(1, tp, lambda k: across(way, j, k).start())
            pl.when(has(way, j))(got)
            start_hop(way, j)

    @named
    def tok_0():
        start_hop(0, 0)
        start_hop(1, 0)

    for j in range(1, A):
        steps[f"tok_{j}"] = lambda j=j: token_step(j)

    @named
    def query_0():
        c_kup.wait()

    def query(i):
        c_wq[i].wait()
        q = dot(xb[a], wqb[:, i * step:(i + 1) * step]).astype(bf16).astype(f32)
        q0, q1, q2 = q[:, :LANES], q[:, LANES:2 * LANES], q[:, 2 * LANES:]
        left = lane < ROPE
        second = jnp.where(left, pltpu.roll(q1, ROPE, 1), pltpu.roll(q2, ROPE, 1))
        ropes = jnp.where(left, q1, q2)
        turned = ropes * cosine[...] + swap_halves(ropes, lane) * sine[...]
        for h, plain, rope in ((0, q0, turned), (1, second, pltpu.roll(turned, ROPE, 1))):
            at = 2 * i + h
            up = kupb[:, at * PLAIN:(at + 1) * PLAIN]
            rows = pl.ds(at * R, R)
            qs[rows, :L] = dot_nt(plain.astype(bf16), up).astype(bf16)
            qs[rows, L:] = rope[:, :ROPE].astype(bf16)

    for i in range(4):
        steps[f"query_{i + 1}"] = lambda i=i: each(
            i, heads // 2 if i == 3 else min(i + 1, heads // 2), query)

    @named
    def keys_own():
        own = xb[a, pl.ds(pl.multiple_of(t * Rk, Rk), Rk)]
        span = D // A
        pre = jnp.zeros((Rk, E), f32)
        for i in range(A):
            pre = pre + dot(own[:, i * span:(i + 1) * span], db[i].reshape(span, E))
        lat = pre[:, :L]
        lat = lat * lax.rsqrt(
            jnp.mean(lat * lat, axis=-1, keepdims=True) + epsilon) * lgain[...]
        rope = jnp.concatenate([pre[:, L:], pre[:, L:]], axis=1)
        krows = pl.ds(pl.multiple_of(t * Rk, Rk), Rk)
        rope = rope * cosine[krows] + swap_halves(rope, lane[:Rk]) * sine[krows]
        kb[a, p.y, p.x, t, :, :L] = lat.astype(bf16)
        kb[a, p.y, p.x, t, :, L:] = rope[:, :ROPE].astype(bf16)

    per = 1
    while per < B2 and (per * 2) * R <= 512 and B2 % (per * 2) == 0:
        per *= 2
    tall = 1
    if per == B2:
        while tall < B1 and (tall * 2) * per * R <= 512 and B1 % (tall * 2) == 0:
            tall *= 2
    KS = tall * per * R
    QR = ROWS if heads * R % ROWS == 0 else R
    blocks = heads * R // QR
    unroll = UNROLL if blocks % UNROLL == 0 else 1
    grade = HEAD ** (-0.5) * 1.4426950408889634

    def each_row(body):
        def some(i, c):
            for u in range(unroll):
                body(i * unroll + u)
            return c
        if blocks == unroll:
            some(0, 0)
        else:
            lax.fori_loop(0, blocks // unroll, some, 0)

    @named
    def attend_init():
        mx[...] = jnp.full(mx.shape, masked_score, f32)
        sm[...] = jnp.zeros(sm.shape, f32)
        acc[...] = jnp.zeros(acc.shape, f32)

    def attend(i, k0, kk, masked):
        rows = pl.ds(pl.multiple_of(i * QR, QR), QR)
        sc = dot_nt(qs[rows], kk)
        if masked:
            at = lax.broadcasted_iota(jnp.int32, (QR, KS), 0)
            kp = lax.broadcasted_iota(jnp.int32, (QR, KS), 1)
            allowed = kp - lax.rem(at, R) <= s * R - k0
            sc = jnp.where(allowed, sc, masked_score)
        old = mx[rows, :1]
        new = jnp.maximum(old, jnp.max(sc, axis=1, keepdims=True))
        w = jnp.exp2((sc - new) * grade)
        fade = jnp.exp2((old - new) * grade)
        sm[rows] = jnp.broadcast_to(
            fade * sm[rows, :1] + jnp.sum(w, axis=1, keepdims=True), (QR, LANES))
        mx[rows] = jnp.broadcast_to(new, (QR, LANES))
        acc[rows] = fade * acc[rows] + dot(w.astype(bf16), kk[:, :L])

    def chunk(k):
        def go():
            c = p.back(k)

            def sub(n):
                y0 = n // (B2 // per) * tall
                x0 = lax.rem(n, B2 // per) * per
                kk = kb[c, pl.ds(y0, tall), pl.ds(x0, per)].reshape(KS, E)
                k0 = (c * B + y0 * B2 + x0) * R
                each_row(lambda i: attend(i, k0, kk, k == 0))
            if B * R == KS:
                sub(0)
            else:
                def maybe(n, q):
                    pl.when(c * B + n * (KS // R) <= s)(lambda: sub(n))
                    return q
                lax.fori_loop(0, B * R // KS, maybe, 0)
        pl.when(k <= a)(go)

    for k in range(A):
        steps[f"attend_{k}"] = lambda k=k: chunk(k)
    NT = 512
    nt = D // NT

    @named
    def attend_out():
        c_vup.wait()
        c_wma.wait()
        top = jnp.zeros((R, LANES), f32)
        total = jnp.ones((R, LANES), f32)
        for h in range(heads):
            rows = pl.ds(h * R, R)
            out = (acc[rows] / sm[rows, :1]).astype(bf16)
            att[:, h * VALUE:(h + 1) * VALUE] = dot(
                out, vupb[:, h * VALUE:(h + 1) * VALUE]).astype(bf16)
            top = jnp.where(lane == h, mx[rows], top)
            total = jnp.where(lane == h, sm[rows], total)
        logs[...] = (top * HEAD ** (-0.5) + jnp.log(total)).T[:heads]

        def attn_merge(n, c):
            cols = pl.ds(pl.multiple_of(n * NT, NT), NT)
            pacc[:, cols] = dot(att[...], wmab[:, cols])
            return c
        lax.fori_loop(0, nt, attn_merge, 0)

    def block(way, j):
        return jnp.clip(a + (2 * way - 1) * j, 0, A - 1)

    def there(place, way, j):
        i = place + (2 * way - 1) * j
        return jnp.logical_and(i >= 0, i < A)

    swap = lambda way, j: remote(
        gated.at[block(way, j)], cb.at[a, pl.ds(HALO, R)], wsend.at[way, j - 1],
        wrecv.at[way, j - 1], p.at(block(way, j), p.y, p.x))

    def after(i):
        return i * B + p.b + 1

    def halo(way, j):
        i = block(way, j)
        to = jnp.minimum(after(i), sp - 1)
        return remote(gated.at[i, pl.ds(R - HALO, HALO)], cb.at[a, pl.ds(0, HALO)],
                      hsend.at[way, j], hrecv.at[way, j], {"sp": to, "tp": t})

    def project(i):
        rows = xb[i]
        v = dot(rows, vb[...].reshape(D, W))
        g = dot(rows, gb[...].reshape(D, W))
        gated[i] = (v / (1.0 + jnp.exp(-g))).astype(bf16)

    def gated_at(j):
        def side(way, c):
            def go():
                each(1, tp, lambda k: across(way, j, k).wait_recv())
                project(block(way, j))
                swap(way, j).start()
                pl.when(after(block(way, j)) < sp)(lambda: halo(way, j).start())
            pl.when(there(a, way, j))(go)
            return c
        lax.fori_loop(0, 2, side, 0)

    for j in range(1, A):
        steps[f"gated_{j}"] = lambda j=j: gated_at(j)

    @named
    def wready():
        c_v.wait()
        c_g.wait()

    @named
    def gated_0():
        project(a)
        cb[a, HALO:] = gated[a]
        pl.when(after(a) < sp)(lambda: halo(0, 0).start())
        pl.when(s == 0)(lambda: cb.__setitem__(
            (slice(None), slice(0, HALO)), jnp.zeros((A, HALO, W), bf16)))

    both_ways = [(way, j) for j in range(1, A) for way in (0, 1)]

    def halos():
        from_line = (s - 1) // B
        halo(0, 0).wait_recv()
        for way, j in both_ways:
            pl.when(there(from_line, 1 - way, j))(
                lambda way=way, j=j: halo(way, j).wait_recv())

    reach = taps.shape[0] - 1
    lead = HALO - reach
    whole = R + HALO
    wb = W // LANES

    def convolve(n, c):
        i = n // wb
        cols = pl.ds(pl.multiple_of(lax.rem(n, wb) * LANES, LANES), LANES)
        full = pl.ds(pl.multiple_of(n * LANES, LANES), LANES)
        xf = cb[i, :, cols].astype(f32)
        tw = taps[:, full].astype(f32)
        out = jnp.zeros((R, LANES), f32)
        for r in range(8):
            xr = xf if r == 0 else pltpu.roll(xf, whole - r, 0)
            for m in range(HALO // 8 + 1):
                j = 8 * m + r - lead
                if 0 <= j <= reach:
                    out = out + tw[j:j + 1] * xr[8 * m:8 * m + R]
        mixed[:, full] = out
        return c

    stats = lambda k: remote(st.at[t], st.at[t], ssend.at[k - 1], srecv.at[k - 1], p.in_tp(k))

    @named
    def conv():
        pl.when(s > 0)(halos)
        for way, j in both_ways:
            pl.when(there(a, 1 - way, j))(lambda way=way, j=j: swap(way, j).wait_recv())
        lax.fori_loop(0, A * wb, convolve, 0)
        all_mixed = mixed[...]
        one = jnp.sum(all_mixed, axis=1, keepdims=True)
        two = jnp.sum(all_mixed * all_mixed, axis=1, keepdims=True)
        st[t] = jnp.where(lane == 0, one, jnp.where(lane == 1, two, 0.0))
        each(1, tp, lambda k: stats(k).start())

    share = lambda n, k: remote(
        pb.at[lax.rem(t + k, tp), :, pl.ds(n * NT, NT)], hold.at[t, :, pl.ds(n * NT, NT)],
        msend.at[n, k - 1], mrecv.at[n, k - 1], p.in_tp(k))

    @named
    def finish():
        each(1, tp, lambda k: stats(k).wait_recv())
        both = jnp.sum(st[...], axis=0)
        mean = both[:, :1] / (C * tp)
        var = both[:, 1:2] / (C * tp) - mean * mean
        z = (mixed[...] - mean) * lax.rsqrt(var + epsilon) * cgain[...]
        out = (z / (1.0 + jnp.exp(-z))).astype(bf16)
        c_wmc.wait()
        for n in range(nt):
            cols = slice(n * NT, (n + 1) * NT)
            part = (dot(out, wmcb[:, cols]) + pacc[:, cols]).astype(bf16)
            for j in range(tp):
                pb[j, :, cols] = part[j * Rk:(j + 1) * Rk]
            each(1, tp, lambda k: share(n, k).start())

    for name in ORDER:
        if name in steps:
            steps[name]()
    keep = pltpu.make_async_copy(pb.at[t], hold.at[t], lsem.at[len(locals_)])
    keep.start()

    each(1, tp, lambda k: tok_pair(k).wait_send())
    for g in (down, keys, value, gate):
        g.drain()
    for way in (0, 1):
        for j in range(A - 1):
            pl.when(jnp.logical_and(has(way, j), onward(way)))(
                lambda way=way, j=j: hop(way, j).wait_send())
        for j in range(1, A):
            pl.when(has(way, j))(lambda way=way, j=j: each(
                1, tp, lambda k: across(way, j, k).wait_send()))
    for way, j in both_ways:
        def sent(way=way, j=j):
            swap(way, j).wait_send()
            pl.when(after(block(way, j)) < sp)(lambda: halo(way, j).wait_send())
        pl.when(there(a, way, j))(sent)
    pl.when(after(a) < sp)(lambda: halo(0, 0).wait_send())
    each(1, tp, lambda k: stats(k).wait_send())
    for n in range(nt):
        each(1, tp, lambda k: share(n, k).wait())
    keep.wait()


def rope_tables(positions):
    lanes = np.arange(LANES)
    inverse = rope_base ** (-2.0 * (lanes % (ROPE // 2)) / ROPE)
    sign = np.where(lanes % ROPE < ROPE // 2, -1.0, 1.0)
    angle = np.asarray(positions, np.float64)[:, None] * inverse[None, :]
    return jnp.asarray(np.stack([np.cos(angle), np.sin(angle) * sign]), f32)


def local(tokens, norm_gain, w_value, w_gate, conv_taps, conv_gain, w_query,
          latent_down_weight, latent_norm_gain, w_rope_key, key_up_weight,
          value_up_weight, w_merge_conv, w_merge_attn):
    R, F = tokens.shape
    sp, tp = lax.axis_size("sp"), lax.axis_size("tp")
    C = w_value.shape[1]
    A = 1
    while A < 4 and sp % (2 * A) == 0 and C % (2 * A * LANES) == 0:
        A *= 2
    B = sp // A
    B2 = 1
    while B2 * B2 < B and B % (2 * B2) == 0:
        B2 *= 2
    B1 = B // B2
    D = w_query.shape[0]
    L = latent_down_weight.shape[1]
    E = L + ROPE
    W = C // A
    Kr = w_value.shape[0]
    heads = w_query.shape[1] // HEAD
    Rk = R // tp
    dtp = tp if Kr % (16 * tp) == 0 else 1
    NT = D // 512
    S = pltpu.SemaphoreType.DMA
    V = pltpu.VMEM
    two = lambda *n: [S(n), S(n)]
    most = max(B1, B2)
    gather = lambda F, G: two(A - 1) + two(A, F - 1) + two(A, F, G - 1)
    by_core = (most, most) if B1 == B2 else (B2, B1)
    sds = jax.ShapeDtypeStruct
    row = lambda v: v.reshape(1, -1)
    hold, logs = pl.pallas_call(
        lambda *refs: kernel(A, B1, B2, tp, dtp, *refs),
        out_shape=(sds((tp, Rk, D), bf16), sds((heads, R), f32)),
        in_specs=[ANY] * 10 + [VMEM] * 6,
        out_specs=(ANY, VMEM),
        scratch_shapes=[
            V((R, LANES), f32), V((R, LANES), f32), V((R, D), bf16), V((A, R, D), bf16),
            V((A, B1, B2, Kr, W), bf16), V((A, B1, B2, Kr, W), bf16),
            V((A, B1, B2, dtp, Kr // dtp, E), bf16), V((A, B1, B2, tp, Rk, E), bf16),
            V((Kr // dtp, L), bf16), V((ROPE, Kr), bf16), V((Kr, ROPE), f32),
            V(w_query.shape, bf16), V(key_up_weight.shape, bf16),
            V(value_up_weight.shape, bf16), V(w_merge_conv.shape, bf16),
            V(w_merge_attn.shape, bf16),
            V((heads * R, E), bf16), V((heads * R, L), f32),
            V((heads * R, LANES), f32), V((heads * R, LANES), f32),
            V((R, heads * VALUE), bf16), V((R, D), f32),
            V((A, R, W), bf16), V((A, R + HALO, W), bf16), V((R, C), f32),
            V((tp, R, LANES), f32), V((tp, Rk, D), bf16),
            S((10 + heads // 2,)), *two(tp - 1), *two(2, A - 1), *two(2, A - 1, tp - 1),
            *gather(*by_core), *two(A, tp - 1), *gather(*by_core), *two(A, tp - 1),
            *gather(B2, B1), *gather(B1, B2),
            *two(2, A - 1), *two(2, A), *two(tp - 1), *two(NT, tp - 1),
        ],
        compiler_params=pltpu.CompilerParams(
            collective_id=0, has_side_effects=True, vmem_limit_bytes=60 * 2**20),
        name="layer",
    )(tokens, w_value, w_gate, w_query, latent_down_weight, w_rope_key.T, key_up_weight,
      value_up_weight, w_merge_conv, w_merge_attn, row(norm_gain), row(latent_norm_gain),
      row(conv_gain), conv_taps, rope_tables(range(R)), rope_tables(range(0, sp * R, R)))
    merged = sum(hold[j].astype(f32) for j in range(tp)).astype(bf16)
    return merged, logs.T


def solution(mesh):
    return jax.shard_map(
        local,
        mesh=mesh,
        in_specs=(
            P("sp", "tp"), P(), P("sp", "tp"), P("sp", "tp"), P(None, "tp"), P("tp"),
            P(None, "tp"), P("sp", None), P(), P("sp", None), P(None, "tp"),
            P(None, "tp"), P("tp", None), P("tp", None),
        ),
        out_specs=(P(("sp", "tp"), None), P("sp", "tp")),
        check_vma=False,
    )
```

```python
import jax
import jax.numpy as jnp
import numpy as np
from jax import lax
from jax.experimental import pallas as pl
from jax.experimental.pallas import tpu as pltpu
from jax.sharding import PartitionSpec as P

PLAIN = 128
ROPE = 64
HEAD = PLAIN + ROPE
VALUE = 128
LANES = 128
HALO = 32

epsilon = 1e-06
rope_base = 10000.0
masked_score = -1e30
MESH = pl.DeviceIdType.MESH
ANY = pl.BlockSpec(memory_space=pltpu.HBM)
VMEM = pl.BlockSpec(memory_space=pltpu.VMEM)
f32, bf16 = jnp.float32, jnp.bfloat16


def each(start, stop, body):
    if stop - start <= 4:
        for k in range(start, stop):
            body(k)
    else:
        lax.fori_loop(start, stop, lambda k, c: (body(k), c)[1], 0)


def dot(a, b):
    return jnp.dot(a, b, preferred_element_type=f32)


def dot_nt(a, b):
    return lax.dot_general(a, b, (((1,), (1,)), ((), ())), preferred_element_type=f32)


ROWS = 1024
UNROLL = 1


ORDER = (
    "down_own", "down_line.3", "down_line.1", "query_0", "gate_spread", "down_line.2",
    "down_2.0", "down_3.0", "gate_line.2", "value_line.1", "down_1.3", "down_1.2",
    "down_1.1", "down_2.3", "tok_start", "value_spread", "value_line.3", "value_line.2",
    "norm", "gate_line.3", "down_2.1", "gate_line.1", "gate_1.2", "rope_own", "down_2.2",
    "tok_0", "down_3.1", "down_4.0", "attend_init", "value_1.3", "value_1.2", "value_1.1",
    "down_3.3", "down_3.2", "down_4.3", "down_4.2", "gate_1.3", "down_4.1", "keys_own",
    "gate_1.1", "keys_line.2", "value_2.3", "keys_spread", "value_2.1", "gate_2.1",
    "keys_line.3", "tok_1", "query_2", "keys_line.1", "keys_2.0", "query_1", "keys_1.2",
    "keys_2.2", "keys_3.0", "gate_2.3", "value_2.0", "gate_2.2", "gate_2.0", "value_2.2",
    "keys_1.3", "query_3", "tok_2", "value_3.0", "value_3.1", "keys_3.2", "keys_4.2",
    "gate_3.2", "value_3.3", "keys_2.3", "keys_1.1", "query_4", "gate_3.1", "gate_3.3",
    "gate_3.0", "value_3.2", "wready", "gated_1", "attend_2", "gated_0", "keys_2.1",
    "keys_4.0", "gated_2", "tok_3", "keys_3.3", "attend_0", "gated_3", "keys_4.3",
    "keys_3.1", "attend_3", "keys_4.1", "attend_1", "conv", "attend_out", "finish",
)


class Place:
    def __init__(self, A, B1, B2, tp):
        self.A, self.B1, self.B2, self.tp = A, B1, B2, tp
        self.B = B1 * B2
        self.sp = A * self.B
        self.s = lax.axis_index("sp")
        self.t = lax.axis_index("tp")
        self.a = self.s // self.B
        self.b = lax.rem(self.s, self.B)
        self.y = self.b // B2
        self.x = lax.rem(self.b, B2)

    def at(self, a, y, x):
        return {"sp": (a * self.B1 + y) * self.B2 + x, "tp": self.t}

    def line(self, k):
        return lax.rem(self.a + k, self.A)

    def back(self, k):
        return lax.rem(self.a + self.A - k, self.A)

    def in_tp(self, k):
        return {"sp": self.s, "tp": lax.rem(self.t + k, self.tp)}


def remote(src, dst, send, recv, where):
    return pltpu.make_async_remote_copy(
        src_ref=src, dst_ref=dst, send_sem=send, recv_sem=recv, device_id=where,
        device_id_type=MESH)


class Gather:
    def __init__(self, p, ref, own, order, sems, paired=None, causal=False):
        self.p, self.ref, self.own, self.order = p, ref, own, order
        self.sl, self.rl, self.sf, self.rf, self.sg, self.rg = sems
        self.paired, self.causal = paired, causal
        if isinstance(order, int):
            self.F, self.G = (p.B2, p.B1) if order else (p.B1, p.B2)
            self.cf, self.cg = (p.x, p.y) if order else (p.y, p.x)
        else:
            assert p.B1 == p.B2
            self.F = self.G = p.B1
            self.cf = p.x * order + p.y * (1 - order)
            self.cg = p.y * order + p.x * (1 - order)

    def only(self, wanted, body):
        if self.causal:
            pl.when(wanted)(body)
        else:
            body()

    def start_line(self, k):
        self.only(self.p.a + k < self.p.A, lambda: self.line(k).start())

    def yx(self, cf, cg):
        o = self.order
        if isinstance(o, int):
            return (cg, cf) if o else (cf, cg)
        return cg * o + cf * (1 - o), cf * o + cg * (1 - o)

    def piece(self, k, jf, jg):
        cf = lax.rem(self.cf + self.F - jf, self.F)
        cg = lax.rem(self.cg + self.G - jg, self.G)
        return self.ref(self.p.back(k), *self.yx(cf, cg))

    def line(self, k):
        p = self.p
        return remote(self.own(k), self.piece(0, 0, 0), self.sl.at[k - 1], self.rl.at[k - 1],
                      p.at(p.line(k), p.y, p.x))

    def source(self, k, jf):
        if isinstance(k, int) and isinstance(jf, int) and k == 0 and jf == 0:
            return self.own(0)
        return self.piece(k, jf, 0)

    def first(self, k, j):
        p = self.p
        to = self.yx(lax.rem(self.cf + j, self.F), self.cg)
        return remote(self.source(k, 0), self.piece(k, 0, 0), self.sf.at[k, j - 1],
                      self.rf.at[k, j - 1], p.at(p.a, *to))

    def second(self, k, jf, j):
        p = self.p
        to = self.yx(self.cf, lax.rem(self.cg + j, self.G))
        return remote(self.source(k, jf), self.piece(k, jf, 0), self.sg.at[k, jf, j - 1],
                      self.rg.at[k, jf, j - 1], p.at(p.a, *to))

    def spread(self, k):
        each(1, self.F, lambda j: self.first(k, j).start())
        each(1, self.G, lambda j: self.second(k, 0, j).start())

    def on_line(self, k):
        def go():
            self.line(k).wait_recv()
            self.spread(k)
        self.only(k <= self.p.a, go)

    def on_first(self, k):
        def arrived(jf):
            self.first(k, jf).wait_recv()
            each(1, self.G, lambda j: self.second(k, jf, j).start())
        self.only(k <= self.p.a, lambda: each(1, self.F, arrived))

    def on_second(self, k):
        def go():
            each(0, self.F, lambda jf: each(
                1, self.G, lambda j: self.second(k, jf, j).wait_recv()))
            if self.paired is not None:
                each(1, self.p.tp, lambda j: self.pair(k, j).start())
        self.only(k <= self.p.a, go)

    def pair(self, k, j):
        whole, send, recv = self.paired
        here = whole(self.p.back(k))
        return remote(here, here, send.at[k, j - 1], recv.at[k, j - 1], self.p.in_tp(j))

    def on_pair(self, k):
        if self.paired is not None:
            self.only(k <= self.p.a, lambda: each(
                1, self.p.tp, lambda j: self.pair(k, j).wait_recv()))

    def drain(self):
        p = self.p
        each(1, p.A, lambda k: self.only(
            p.a + k < p.A, lambda: self.line(k).wait_send()))

        def out(k):
            def go():
                each(1, self.F, lambda j: self.first(k, j).wait_send())
                each(0, self.F, lambda jf: each(
                    1, self.G, lambda j: self.second(k, jf, j).wait_send()))
                if self.paired is not None:
                    each(1, p.tp, lambda j: self.pair(k, j).wait_send())
            self.only(k <= p.a, go)
        each(0, p.A, out)


def swap_halves(v, lane):
    low = lax.rem(lane, ROPE) < ROPE // 2
    return jnp.where(low, pltpu.roll(v, LANES - ROPE // 2, 1), pltpu.roll(v, ROPE // 2, 1))


def kernel(A, B1, B2, tp, dtp,
           tok, wv, wg, wq, ld, wr, kup, vup, wmc, wma,
           gain, lgain, cgain, taps, near, far,
           hold, logs,
           cosine, sine, xin, xb, vb, gb, db, kb, dl, dr, drt, wqb, kupb, vupb, wmcb, wmab, qs, acc, mx, sm,
           att, pacc, gated, cb, mixed, st, pb,
           lsem, tsend, trecv, zsend, zrecv, psend, precv,
           dls, dlr, dfs, dfr, dgs, dgr, dps, dpr,
           kls, klr, kfs, kfr, kgs, kgr, kps, kpr,
           vls, vlr, vfs, vfr, vgs, vgr,
           gls, glr, gfs, gfr, ggs, ggr,
           wsend, wrecv, hsend, hrecv, ssend, srecv, msend, mrecv):
    p = Place(A, B1, B2, tp)
    B, sp, a, s, t = p.B, p.sp, p.a, p.s, p.t
    R, F = tok.shape
    D = wq.shape[0]
    L = ld.shape[1]
    E = L + ROPE
    C = wv.shape[1]
    W = C // A
    heads = wq.shape[1] // HEAD
    Rk = R // tp
    mine = pl.ds(pl.multiple_of(t * F, F), F)
    columns = lambda k: pl.ds(pl.multiple_of(p.line(k) * W, W), W)

    locals_ = []

    def load(src, dst):
        c = pltpu.make_async_copy(src, dst, lsem.at[len(locals_)])
        locals_.append(c)
        c.start()
        return c

    drows = ld.shape[0] // dtp
    td = t if dtp > 1 else 0
    dpart = pl.ds(pl.multiple_of(td * drows, drows), drows)
    c_tok = load(tok, xin.at[:, mine])
    c_ld = load(ld.at[dpart], dl)
    c_wr = load(wr, dr)
    c_v = load(wv.at[:, columns(0)], vb.at[a, p.y, p.x])
    c_g = load(wg.at[:, columns(0)], gb.at[a, p.y, p.x])
    step = 2 * HEAD
    c_wq = [load(wq.at[:, pl.ds(i * step, step)], wqb.at[:, pl.ds(i * step, step)])
            for i in range(heads // 2)]
    c_kup = load(kup, kupb)
    c_vup = load(vup, vupb)
    c_wma = load(wma, wmab)
    c_wmc = load(wmc, wmcb)

    barrier = pltpu.get_barrier_semaphore()
    lax.fori_loop(1, sp, lambda k, c: (pl.semaphore_signal(
        barrier, inc=1, device_id={"sp": lax.rem(s + k, sp), "tp": t},
        device_id_type=MESH), c)[1], 0)
    lax.fori_loop(1, tp, lambda k, c: (pl.semaphore_signal(
        barrier, inc=1, device_id=p.in_tp(k), device_id_type=MESH), c)[1], 0)
    pl.semaphore_wait(barrier, sp - 1 + tp - 1)

    by_core = 1 - lax.rem(t, 2) if B1 == B2 else 1
    down = Gather(p, lambda i, y, x: db.at[i, y, x, td],
                  lambda k: db.at[a, p.y, p.x, td], by_core,
                  (dls, dlr, dfs, dfr, dgs, dgr),
                  (lambda i: db.at[i, :, :, td], dps, dpr) if dtp > 1 else None)
    keys = Gather(p, lambda i, y, x: kb.at[i, y, x, t],
                  lambda k: kb.at[a, p.y, p.x, t], by_core,
                  (kls, klr, kfs, kfr, kgs, kgr),
                  (lambda i: kb.at[i, :, :, t], kps, kpr), causal=True)
    value = Gather(p, lambda i, y, x: vb.at[i, y, x],
                   lambda k: wv.at[:, columns(k)], 1, (vls, vlr, vfs, vfr, vgs, vgr))
    gate = Gather(p, lambda i, y, x: gb.at[i, y, x],
                  lambda k: wg.at[:, columns(k)], 0, (gls, glr, gfs, gfr, ggs, ggr))

    lane = lax.broadcasted_iota(jnp.int32, (R, LANES), 1)
    tok_pair = lambda k: remote(tok, xin.at[:, mine], tsend.at[k - 1], trecv.at[k - 1], p.in_tp(k))
    steps = {}

    def named(f):
        steps[f.__name__] = f
        return f

    @named
    def tok_start():
        each(1, tp, lambda k: tok_pair(k).start())

    @named
    def down_own():
        c_ld.wait()
        c_wr.wait()
        drt[...] = dr[...].astype(f32).T
        db[a, p.y, p.x, td, :, :L] = dl[...]
        db[a, p.y, p.x, td, :, L:] = drt[dpart].astype(bf16)
        down.spread(0)

    for name, g in (("down", down), ("keys", keys), ("value", value), ("gate", gate)):
        steps[name + "_spread"] = lambda g=g: g.spread(0)
        for k in range(A):
            if k:
                steps[f"{name}_line.{k}"] = lambda g=g, k=k: g.start_line(k)
                steps[f"{name}_1.{k}"] = lambda g=g, k=k: g.on_line(k)
            steps[f"{name}_2.{k}"] = lambda g=g, k=k: g.on_first(k)
            steps[f"{name}_3.{k}"] = lambda g=g, k=k: g.on_second(k)
            steps[f"{name}_4.{k}"] = lambda g=g, k=k: g.on_pair(k)

    NR = 32 if R % 32 == 0 else R

    @named
    def norm():
        c_tok.wait()
        each(1, tp, lambda k: tok_pair(k).wait_recv())

        def rows_norm(i, c):
            rows = pl.ds(pl.multiple_of(i * NR, NR), NR)
            v = xin[rows].astype(f32)
            scale = lax.rsqrt(jnp.mean(v * v, axis=-1, keepdims=True) + epsilon)
            xb[a, rows] = (v * scale * gain[...]).astype(bf16)
            return c
        lax.fori_loop(0, R // NR, rows_norm, 0)

    @named
    def rope_own():
        c0, s0 = far[0, pl.ds(s, 1)], far[1, pl.ds(s, 1)]
        cosine[...] = near[0] * c0 - near[1] * s0
        sine[...] = near[1] * c0 + near[0] * s0

    def hop(way, j):
        i = jnp.clip(a + (-j if way == 0 else j), 0, A - 1)
        to = jnp.clip(a + (1 if way == 0 else -1), 0, A - 1)
        return remote(xb.at[i, :, mine], xb.at[i, :, mine], zsend.at[way, j],
                      zrecv.at[way, j], p.at(to, p.y, p.x))

    def across(way, j, k):
        i = jnp.clip(a + (2 * way - 1) * j, 0, A - 1)
        return remote(xb.at[i, :, mine], xb.at[i, :, mine], psend.at[way, j - 1, k - 1],
                      precv.at[way, j - 1, k - 1], p.in_tp(k))

    def has(way, j):
        return a - j >= 0 if way == 0 else a + j < A

    def onward(way):
        return a + 1 < A if way == 0 else a >= 1

    def start_hop(way, j):
        if j < A - 1:
            pl.when(jnp.logical_and(has(way, j), onward(way)))(lambda: hop(way, j).start())

    def token_step(j):
        for way in (0, 1):
            def got(way=way):
                hop(way, j - 1).wait_recv()
                each(1, tp, lambda k: across(way, j, k).start())
            pl.when(has(way, j))(got)
            start_hop(way, j)

    @named
    def tok_0():
        start_hop(0, 0)
        start_hop(1, 0)

    for j in range(1, A):
        steps[f"tok_{j}"] = lambda j=j: token_step(j)

    @named
    def query_0():
        c_kup.wait()

    def query(i):
        c_wq[i].wait()
        q = dot(xb[a], wqb[:, i * step:(i + 1) * step]).astype(bf16).astype(f32)
        q0, q1, q2 = q[:, :LANES], q[:, LANES:2 * LANES], q[:, 2 * LANES:]
        left = lane < ROPE
        second = jnp.where(left, pltpu.roll(q1, ROPE, 1), pltpu.roll(q2, ROPE, 1))
        ropes = jnp.where(left, q1, q2)
        turned = ropes * cosine[...] + swap_halves(ropes, lane) * sine[...]
        for h, plain, rope in ((0, q0, turned), (1, second, pltpu.roll(turned, ROPE, 1))):
            at = 2 * i + h
            up = kupb[:, at * PLAIN:(at + 1) * PLAIN]
            rows = pl.ds(at * R, R)
            qs[:L, rows] = dot_nt(up, plain.astype(bf16)).astype(bf16)
            qs[L:, rows] = rope.T[:ROPE].astype(bf16)

    for i in range(4):
        steps[f"query_{i + 1}"] = lambda i=i: each(
            i, heads // 2 if i == 3 else min(i + 1, heads // 2), query)

    @named
    def keys_own():
        own = xb[a, pl.ds(pl.multiple_of(t * Rk, Rk), Rk)]
        span = D // A
        pre = jnp.zeros((Rk, E), f32)
        for i in range(A):
            pre = pre + dot(own[:, i * span:(i + 1) * span], db[i].reshape(span, E))
        lat = pre[:, :L]
        lat = lat * lax.rsqrt(
            jnp.mean(lat * lat, axis=-1, keepdims=True) + epsilon) * lgain[...]
        rope = jnp.concatenate([pre[:, L:], pre[:, L:]], axis=1)
        krows = pl.ds(pl.multiple_of(t * Rk, Rk), Rk)
        rope = rope * cosine[krows] + swap_halves(rope, lane[:Rk]) * sine[krows]
        kb[a, p.y, p.x, t, :, :L] = lat.astype(bf16)
        kb[a, p.y, p.x, t, :, L:] = rope[:, :ROPE].astype(bf16)

    per = 1
    while per < B2 and (per * 2) * R <= 512 and B2 % (per * 2) == 0:
        per *= 2
    tall = 1
    if per == B2:
        while tall < B1 and (tall * 2) * per * R <= 512 and B1 % (tall * 2) == 0:
            tall *= 2
    KS = tall * per * R
    QR = ROWS if heads * R % ROWS == 0 else R
    blocks = heads * R // QR
    unroll = UNROLL if blocks % UNROLL == 0 else 1
    grade = HEAD ** (-0.5) * 1.4426950408889634

    def each_row(body):
        def some(i, c):
            for u in range(unroll):
                body(i * unroll + u)
            return c
        if blocks == unroll:
            some(0, 0)
        else:
            lax.fori_loop(0, blocks // unroll, some, 0)

    @named
    def attend_init():
        mx[...] = jnp.full(mx.shape, masked_score, f32)
        sm[...] = jnp.zeros(sm.shape, f32)
        acc[...] = jnp.zeros(acc.shape, f32)

    def attend(i, k0, kk, kt, masked):
        rows = pl.ds(pl.multiple_of(i * QR, QR), QR)
        sc = dot(kk, qs[:, rows])
        if masked:
            kp = lax.broadcasted_iota(jnp.int32, (KS, QR), 0)
            at = lax.broadcasted_iota(jnp.int32, (KS, QR), 1)
            allowed = kp - lax.rem(at, R) <= s * R - k0
            sc = jnp.where(allowed, sc, masked_score)
        old = mx[:, rows]
        new = jnp.maximum(old, jnp.max(sc, axis=0, keepdims=True))
        w = jnp.exp2((sc - new) * grade)
        fade = jnp.exp2((old - new) * grade)
        sm[:, rows] = fade * sm[:, rows] + jnp.sum(w, axis=0, keepdims=True)
        mx[:, rows] = new
        acc[:, rows] = fade * acc[:, rows] + dot(kt, w.astype(bf16))

    def chunk(k):
        def go():
            c = p.back(k)

            def sub(n):
                y0 = n // (B2 // per) * tall
                x0 = lax.rem(n, B2 // per) * per
                kk = kb[c, pl.ds(y0, tall), pl.ds(x0, per)].reshape(KS, E)
                k0 = (c * B + y0 * B2 + x0) * R
                kt = kk[:, :L].T
                each_row(lambda i: attend(i, k0, kk, kt, k == 0))
            if B * R == KS:
                sub(0)
            else:
                def maybe(n, q):
                    pl.when(c * B + n * (KS // R) <= s)(lambda: sub(n))
                    return q
                lax.fori_loop(0, B * R // KS, maybe, 0)
        pl.when(k <= a)(go)

    for k in range(A):
        steps[f"attend_{k}"] = lambda k=k: chunk(k)
    NT = 512
    nt = D // NT

    @named
    def attend_out():
        c_vup.wait()
        c_wma.wait()
        for h in range(heads):
            rows = pl.ds(h * R, R)
            out = (acc[:, rows] / sm[:, rows]).T.astype(bf16)
            att[:, h * VALUE:(h + 1) * VALUE] = dot(
                out, vupb[:, h * VALUE:(h + 1) * VALUE]).astype(bf16)
            logs[h:h + 1] = mx[:, rows] * HEAD ** (-0.5) + jnp.log(sm[:, rows])

        def attn_merge(n, c):
            cols = pl.ds(pl.multiple_of(n * NT, NT), NT)
            pacc[:, cols] = dot(att[...], wmab[:, cols])
            return c
        lax.fori_loop(0, nt, attn_merge, 0)

    def block(way, j):
        return jnp.clip(a + (2 * way - 1) * j, 0, A - 1)

    def there(place, way, j):
        i = place + (2 * way - 1) * j
        return jnp.logical_and(i >= 0, i < A)

    swap = lambda way, j: remote(
        gated.at[block(way, j)], cb.at[a, pl.ds(HALO, R)], wsend.at[way, j - 1],
        wrecv.at[way, j - 1], p.at(block(way, j), p.y, p.x))

    def after(i):
        return i * B + p.b + 1

    def halo(way, j):
        i = block(way, j)
        to = jnp.minimum(after(i), sp - 1)
        return remote(gated.at[i, pl.ds(R - HALO, HALO)], cb.at[a, pl.ds(0, HALO)],
                      hsend.at[way, j], hrecv.at[way, j], {"sp": to, "tp": t})

    def project(i):
        rows = xb[i]
        v = dot(rows, vb[...].reshape(D, W))
        g = dot(rows, gb[...].reshape(D, W))
        gated[i] = (v / (1.0 + jnp.exp(-g))).astype(bf16)

    def gated_at(j):
        def side(way, c):
            def go():
                each(1, tp, lambda k: across(way, j, k).wait_recv())
                project(block(way, j))
                swap(way, j).start()
                pl.when(after(block(way, j)) < sp)(lambda: halo(way, j).start())
            pl.when(there(a, way, j))(go)
            return c
        lax.fori_loop(0, 2, side, 0)

    for j in range(1, A):
        steps[f"gated_{j}"] = lambda j=j: gated_at(j)

    @named
    def wready():
        c_v.wait()
        c_g.wait()

    @named
    def gated_0():
        project(a)
        cb[a, HALO:] = gated[a]
        pl.when(after(a) < sp)(lambda: halo(0, 0).start())
        pl.when(s == 0)(lambda: cb.__setitem__(
            (slice(None), slice(0, HALO)), jnp.zeros((A, HALO, W), bf16)))

    both_ways = [(way, j) for j in range(1, A) for way in (0, 1)]

    def halos():
        from_line = (s - 1) // B
        halo(0, 0).wait_recv()
        for way, j in both_ways:
            pl.when(there(from_line, 1 - way, j))(
                lambda way=way, j=j: halo(way, j).wait_recv())

    reach = taps.shape[0] - 1
    lead = HALO - reach
    whole = R + HALO
    wb = W // LANES

    def convolve(n, c):
        i = n // wb
        cols = pl.ds(pl.multiple_of(lax.rem(n, wb) * LANES, LANES), LANES)
        full = pl.ds(pl.multiple_of(n * LANES, LANES), LANES)
        xf = cb[i, :, cols].astype(f32)
        tw = taps[:, full].astype(f32)
        out = jnp.zeros((R, LANES), f32)
        for r in range(8):
            xr = xf if r == 0 else pltpu.roll(xf, whole - r, 0)
            for m in range(HALO // 8 + 1):
                j = 8 * m + r - lead
                if 0 <= j <= reach:
                    out = out + tw[j:j + 1] * xr[8 * m:8 * m + R]
        mixed[:, full] = out
        return c

    stats = lambda k: remote(st.at[t], st.at[t], ssend.at[k - 1], srecv.at[k - 1], p.in_tp(k))

    @named
    def conv():
        pl.when(s > 0)(halos)
        for way, j in both_ways:
            pl.when(there(a, 1 - way, j))(lambda way=way, j=j: swap(way, j).wait_recv())
        lax.fori_loop(0, A * wb, convolve, 0)
        all_mixed = mixed[...]
        one = jnp.sum(all_mixed, axis=1, keepdims=True)
        two = jnp.sum(all_mixed * all_mixed, axis=1, keepdims=True)
        st[t] = jnp.where(lane == 0, one, jnp.where(lane == 1, two, 0.0))
        each(1, tp, lambda k: stats(k).start())

    share = lambda n, k: remote(
        pb.at[lax.rem(t + k, tp), :, pl.ds(n * NT, NT)], hold.at[t, :, pl.ds(n * NT, NT)],
        msend.at[n, k - 1], mrecv.at[n, k - 1], p.in_tp(k))

    @named
    def finish():
        each(1, tp, lambda k: stats(k).wait_recv())
        both = jnp.sum(st[...], axis=0)
        mean = both[:, :1] / (C * tp)
        var = both[:, 1:2] / (C * tp) - mean * mean
        z = (mixed[...] - mean) * lax.rsqrt(var + epsilon) * cgain[...]
        out = (z / (1.0 + jnp.exp(-z))).astype(bf16)
        c_wmc.wait()
        for n in range(nt):
            cols = slice(n * NT, (n + 1) * NT)
            part = (dot(out, wmcb[:, cols]) + pacc[:, cols]).astype(bf16)
            for j in range(tp):
                pb[j, :, cols] = part[j * Rk:(j + 1) * Rk]
            each(1, tp, lambda k: share(n, k).start())

    for name in ORDER:
        if name in steps:
            steps[name]()
    hold[t] = pb[t]

    each(1, tp, lambda k: tok_pair(k).wait_send())
    for g in (down, keys, value, gate):
        g.drain()
    for way in (0, 1):
        for j in range(A - 1):
            pl.when(jnp.logical_and(has(way, j), onward(way)))(
                lambda way=way, j=j: hop(way, j).wait_send())
        for j in range(1, A):
            pl.when(has(way, j))(lambda way=way, j=j: each(
                1, tp, lambda k: across(way, j, k).wait_send()))
    for way, j in both_ways:
        def sent(way=way, j=j):
            swap(way, j).wait_send()
            pl.when(after(block(way, j)) < sp)(lambda: halo(way, j).wait_send())
        pl.when(there(a, way, j))(sent)
    pl.when(after(a) < sp)(lambda: halo(0, 0).wait_send())
    each(1, tp, lambda k: stats(k).wait_send())
    for n in range(nt):
        each(1, tp, lambda k: share(n, k).wait())


def total_kernel(hold, logs, merged, log_sums):
    whole_sum = hold[0].astype(f32)
    for j in range(1, hold.shape[0]):
        whole_sum = whole_sum + hold[j].astype(f32)
    merged[...] = whole_sum.astype(bf16)
    log_sums[...] = logs[...]


def rope_tables(positions):
    lanes = np.arange(LANES)
    inverse = rope_base ** (-2.0 * (lanes % (ROPE // 2)) / ROPE)
    sign = np.where(lanes % ROPE < ROPE // 2, -1.0, 1.0)
    angle = np.asarray(positions, np.float64)[:, None] * inverse[None, :]
    return jnp.asarray(np.stack([np.cos(angle), np.sin(angle) * sign]), f32)


def local(tokens, norm_gain, w_value, w_gate, conv_taps, conv_gain, w_query,
          latent_down_weight, latent_norm_gain, w_rope_key, key_up_weight,
          value_up_weight, w_merge_conv, w_merge_attn):
    R, F = tokens.shape
    sp, tp = lax.axis_size("sp"), lax.axis_size("tp")
    C = w_value.shape[1]
    A = 1
    while A < 4 and sp % (2 * A) == 0 and C % (2 * A * LANES) == 0:
        A *= 2
    B = sp // A
    B2 = 1
    while B2 * B2 < B and B % (2 * B2) == 0:
        B2 *= 2
    B1 = B // B2
    D = w_query.shape[0]
    L = latent_down_weight.shape[1]
    E = L + ROPE
    W = C // A
    Kr = w_value.shape[0]
    heads = w_query.shape[1] // HEAD
    Rk = R // tp
    dtp = tp if Kr % (16 * tp) == 0 else 1
    NT = D // 512
    S = pltpu.SemaphoreType.DMA
    V = pltpu.VMEM
    two = lambda *n: [S(n), S(n)]
    most = max(B1, B2)
    gather = lambda F, G: two(A - 1) + two(A, F - 1) + two(A, F, G - 1)
    by_core = (most, most) if B1 == B2 else (B2, B1)
    sds = jax.ShapeDtypeStruct
    row = lambda v: v.reshape(1, -1)
    hold, logs = pl.pallas_call(
        lambda *refs: kernel(A, B1, B2, tp, dtp, *refs),
        out_shape=(V((tp, Rk, D), bf16), V((heads, R), f32)),
        in_specs=[ANY] * 10 + [VMEM] * 6,
        out_specs=(VMEM, VMEM),
        scratch_shapes=[
            V((R, LANES), f32), V((R, LANES), f32), V((R, D), bf16), V((A, R, D), bf16),
            V((A, B1, B2, Kr, W), bf16), V((A, B1, B2, Kr, W), bf16),
            V((A, B1, B2, dtp, Kr // dtp, E), bf16), V((A, B1, B2, tp, Rk, E), bf16),
            V((Kr // dtp, L), bf16), V((ROPE, Kr), bf16), V((Kr, ROPE), f32),
            V(w_query.shape, bf16), V(key_up_weight.shape, bf16),
            V(value_up_weight.shape, bf16), V(w_merge_conv.shape, bf16),
            V(w_merge_attn.shape, bf16),
            V((E, heads * R), bf16), V((L, heads * R), f32),
            V((1, heads * R), f32), V((1, heads * R), f32),
            V((R, heads * VALUE), bf16), V((R, D), f32),
            V((A, R, W), bf16), V((A, R + HALO, W), bf16), V((R, C), f32),
            V((tp, R, LANES), f32), V((tp, Rk, D), bf16),
            S((10 + heads // 2,)), *two(tp - 1), *two(2, A - 1), *two(2, A - 1, tp - 1),
            *gather(*by_core), *two(A, tp - 1), *gather(*by_core), *two(A, tp - 1),
            *gather(B2, B1), *gather(B1, B2),
            *two(2, A - 1), *two(2, A), *two(tp - 1), *two(NT, tp - 1),
        ],
        compiler_params=pltpu.CompilerParams(
            collective_id=0, has_side_effects=True, vmem_limit_bytes=60 * 2**20),
        name="layer",
    )(*(pltpu.with_memory_space_constraint(v, pltpu.HBM) for v in (
        tokens, w_value, w_gate, w_query, latent_down_weight, w_rope_key.T, key_up_weight,
        value_up_weight, w_merge_conv, w_merge_attn)), row(norm_gain), row(latent_norm_gain),
      row(conv_gain), conv_taps, rope_tables(range(R)), rope_tables(range(0, sp * R, R)))
    merged, logs = pl.pallas_call(
        total_kernel,
        out_shape=(sds((Rk, D), bf16), sds((heads, R), f32)),
        in_specs=[VMEM] * 2,
        out_specs=(VMEM,) * 2,
        compiler_params=pltpu.CompilerParams(vmem_limit_bytes=4 * 2**20),
        name="total",
    )(hold, logs)
    return merged, logs.T


def solution(mesh):
    return jax.shard_map(
        local,
        mesh=mesh,
        in_specs=(
            P("sp", "tp"), P(), P("sp", "tp"), P("sp", "tp"), P(None, "tp"), P("tp"),
            P(None, "tp"), P("sp", None), P(), P("sp", None), P(None, "tp"),
            P(None, "tp"), P("tp", None), P("tp", None),
        ),
        out_specs=(P(("sp", "tp"), None), P("sp", "tp")),
        check_vma=False,
    )
```

```python
import jax
import jax.numpy as jnp
import numpy as np
from jax import lax
from jax.experimental import pallas as pl
from jax.experimental.pallas import tpu as pltpu
from jax.sharding import PartitionSpec as P

PLAIN = 128
ROPE = 64
HEAD = PLAIN + ROPE
VALUE = 128
LANES = 128
HALO = 32

epsilon = 1e-06
rope_base = 10000.0
masked_score = -1e30
MESH = pl.DeviceIdType.MESH
ANY = pl.BlockSpec(memory_space=pltpu.HBM)
VMEM = pl.BlockSpec(memory_space=pltpu.VMEM)
f32, bf16 = jnp.float32, jnp.bfloat16


def each(start, stop, body):
    if stop - start <= 4:
        for k in range(start, stop):
            body(k)
    else:
        lax.fori_loop(start, stop, lambda k, c: (body(k), c)[1], 0)


def dot(a, b):
    return jnp.dot(a, b, preferred_element_type=f32)


def dot_nt(a, b):
    return lax.dot_general(a, b, (((1,), (1,)), ((), ())), preferred_element_type=f32)


ROWS = 1024
UNROLL = 1


ORDER = (
    "down_own", "down_line.3", "down_line.1", "query_0", "gate_spread", "down_line.2",
    "down_2.0", "down_3.0", "gate_line.2", "value_line.1", "down_1.3", "down_1.2",
    "down_1.1", "down_2.3", "tok_start", "value_spread", "value_line.3", "value_line.2",
    "norm", "gate_line.3", "down_2.1", "gate_line.1", "gate_1.2", "down_2.2", "tok_0",
    "down_3.1", "down_4.0", "attend_init", "rope_own", "value_1.3", "value_1.2",
    "value_1.1", "down_3.3", "down_3.2", "down_4.3", "down_4.2", "gate_1.3", "down_4.1",
    "keys_own", "gate_1.1", "keys_line.2", "value_2.3", "keys_spread", "value_2.1",
    "gate_2.1", "keys_line.3", "tok_1", "query_2", "keys_line.1", "keys_2.0", "query_1",
    "keys_1.2", "keys_2.2", "keys_3.0", "gate_2.3", "value_2.0", "gate_2.2", "gate_2.0",
    "value_2.2", "keys_1.3", "query_3", "tok_2", "value_3.0", "value_3.1", "keys_3.2",
    "keys_4.2", "gate_3.2", "value_3.3", "keys_2.3", "keys_1.1", "query_4", "gate_3.1",
    "gate_3.3", "gate_3.0", "value_3.2", "wready", "gated_1", "attend_2", "gated_0",
    "keys_2.1", "keys_4.0", "gated_2", "tok_3", "keys_3.3", "attend_0", "gated_3",
    "keys_4.3", "keys_3.1", "attend_3", "keys_4.1", "attend_1", "attend_out", "conv",
    "finish",
)


class Place:
    def __init__(self, A, B1, B2, tp):
        self.A, self.B1, self.B2, self.tp = A, B1, B2, tp
        self.B = B1 * B2
        self.sp = A * self.B
        self.s = lax.axis_index("sp")
        self.t = lax.axis_index("tp")
        self.a = self.s // self.B
        self.b = lax.rem(self.s, self.B)
        self.y = self.b // B2
        self.x = lax.rem(self.b, B2)

    def at(self, a, y, x):
        return {"sp": (a * self.B1 + y) * self.B2 + x, "tp": self.t}

    def line(self, k):
        return lax.rem(self.a + k, self.A)

    def back(self, k):
        return lax.rem(self.a + self.A - k, self.A)

    def in_tp(self, k):
        return {"sp": self.s, "tp": lax.rem(self.t + k, self.tp)}


def remote(src, dst, send, recv, where):
    return pltpu.make_async_remote_copy(
        src_ref=src, dst_ref=dst, send_sem=send, recv_sem=recv, device_id=where,
        device_id_type=MESH)


class Gather:
    def __init__(self, p, ref, own, order, sems, paired=None, causal=False):
        self.p, self.ref, self.own, self.order = p, ref, own, order
        self.sl, self.rl, self.sf, self.rf, self.sg, self.rg = sems
        self.paired, self.causal = paired, causal
        if isinstance(order, int):
            self.F, self.G = (p.B2, p.B1) if order else (p.B1, p.B2)
            self.cf, self.cg = (p.x, p.y) if order else (p.y, p.x)
        else:
            assert p.B1 == p.B2
            self.F = self.G = p.B1
            self.cf = p.x * order + p.y * (1 - order)
            self.cg = p.y * order + p.x * (1 - order)

    def only(self, wanted, body):
        if self.causal:
            pl.when(wanted)(body)
        else:
            body()

    def start_line(self, k):
        self.only(self.p.a + k < self.p.A, lambda: self.line(k).start())

    def yx(self, cf, cg):
        o = self.order
        if isinstance(o, int):
            return (cg, cf) if o else (cf, cg)
        return cg * o + cf * (1 - o), cf * o + cg * (1 - o)

    def piece(self, k, jf, jg):
        cf = lax.rem(self.cf + self.F - jf, self.F)
        cg = lax.rem(self.cg + self.G - jg, self.G)
        return self.ref(self.p.back(k), *self.yx(cf, cg))

    def line(self, k):
        p = self.p
        return remote(self.own(k), self.piece(0, 0, 0), self.sl.at[k - 1], self.rl.at[k - 1],
                      p.at(p.line(k), p.y, p.x))

    def source(self, k, jf):
        if isinstance(k, int) and isinstance(jf, int) and k == 0 and jf == 0:
            return self.own(0)
        return self.piece(k, jf, 0)

    def first(self, k, j):
        p = self.p
        to = self.yx(lax.rem(self.cf + j, self.F), self.cg)
        return remote(self.source(k, 0), self.piece(k, 0, 0), self.sf.at[k, j - 1],
                      self.rf.at[k, j - 1], p.at(p.a, *to))

    def second(self, k, jf, j):
        p = self.p
        to = self.yx(self.cf, lax.rem(self.cg + j, self.G))
        return remote(self.source(k, jf), self.piece(k, jf, 0), self.sg.at[k, jf, j - 1],
                      self.rg.at[k, jf, j - 1], p.at(p.a, *to))

    def spread(self, k):
        each(1, self.F, lambda j: self.first(k, j).start())
        each(1, self.G, lambda j: self.second(k, 0, j).start())

    def on_line(self, k):
        def go():
            self.line(k).wait_recv()
            self.spread(k)
        self.only(k <= self.p.a, go)

    def on_first(self, k):
        def arrived(jf):
            self.first(k, jf).wait_recv()
            each(1, self.G, lambda j: self.second(k, jf, j).start())
        self.only(k <= self.p.a, lambda: each(1, self.F, arrived))

    def on_second(self, k):
        def go():
            each(0, self.F, lambda jf: each(
                1, self.G, lambda j: self.second(k, jf, j).wait_recv()))
            if self.paired is not None:
                each(1, self.p.tp, lambda j: self.pair(k, j).start())
        self.only(k <= self.p.a, go)

    def pair(self, k, j):
        whole, send, recv = self.paired
        here = whole(self.p.back(k))
        return remote(here, here, send.at[k, j - 1], recv.at[k, j - 1], self.p.in_tp(j))

    def on_pair(self, k):
        if self.paired is not None:
            self.only(k <= self.p.a, lambda: each(
                1, self.p.tp, lambda j: self.pair(k, j).wait_recv()))

    def drain(self):
        p = self.p
        each(1, p.A, lambda k: self.only(
            p.a + k < p.A, lambda: self.line(k).wait_send()))

        def out(k):
            def go():
                each(1, self.F, lambda j: self.first(k, j).wait_send())
                each(0, self.F, lambda jf: each(
                    1, self.G, lambda j: self.second(k, jf, j).wait_send()))
                if self.paired is not None:
                    each(1, p.tp, lambda j: self.pair(k, j).wait_send())
            self.only(k <= p.a, go)
        each(0, p.A, out)


def swap_halves(v, lane):
    low = lax.rem(lane, ROPE) < ROPE // 2
    return jnp.where(low, pltpu.roll(v, LANES - ROPE // 2, 1), pltpu.roll(v, ROPE // 2, 1))


def kernel(A, B1, B2, tp, dtp,
           tok, wv, wg, wq, ld, wr, kup, vup, wmc, wma,
           gain, lgain, cgain, taps, near, far,
           hold, logs,
           cosine, sine, xin, xb, vb, gb, db, kb, dl, dr, drt, wqb, kupb, vupb, wmcb, wmab, qs, acc, mx, sm,
           att, pacc, gated, cb, mixed, st, pb,
           lsem, tsend, trecv, zsend, zrecv, psend, precv,
           dls, dlr, dfs, dfr, dgs, dgr, dps, dpr,
           kls, klr, kfs, kfr, kgs, kgr, kps, kpr,
           vls, vlr, vfs, vfr, vgs, vgr,
           gls, glr, gfs, gfr, ggs, ggr,
           wsend, wrecv, hsend, hrecv, ssend, srecv, msend, mrecv):
    p = Place(A, B1, B2, tp)
    B, sp, a, s, t = p.B, p.sp, p.a, p.s, p.t
    R, F = tok.shape
    D = wq.shape[0]
    L = ld.shape[1]
    E = L + ROPE
    C = wv.shape[1]
    W = C // A
    heads = wq.shape[1] // HEAD
    Rk = R // tp
    mine = pl.ds(pl.multiple_of(t * F, F), F)
    columns = lambda k: pl.ds(pl.multiple_of(p.line(k) * W, W), W)

    locals_ = []

    def load(src, dst):
        c = pltpu.make_async_copy(src, dst, lsem.at[len(locals_)])
        locals_.append(c)
        c.start()
        return c

    drows = ld.shape[0] // dtp
    td = t if dtp > 1 else 0
    dpart = pl.ds(pl.multiple_of(td * drows, drows), drows)
    c_tok = load(tok, xin.at[:, mine])
    c_ld = load(ld.at[dpart], dl)
    c_wr = load(wr, dr)
    c_v = load(wv.at[:, columns(0)], vb.at[a, p.y, p.x])
    c_g = load(wg.at[:, columns(0)], gb.at[a, p.y, p.x])
    step = 2 * HEAD
    c_wq = [load(wq.at[:, pl.ds(i * step, step)], wqb.at[:, pl.ds(i * step, step)])
            for i in range(heads // 2)]
    c_kup = load(kup, kupb)
    c_vup = load(vup, vupb)
    c_wma = load(wma, wmab)
    c_wmc = load(wmc, wmcb)

    barrier = pltpu.get_barrier_semaphore()
    lax.fori_loop(1, sp, lambda k, c: (pl.semaphore_signal(
        barrier, inc=1, device_id={"sp": lax.rem(s + k, sp), "tp": t},
        device_id_type=MESH), c)[1], 0)
    lax.fori_loop(1, tp, lambda k, c: (pl.semaphore_signal(
        barrier, inc=1, device_id=p.in_tp(k), device_id_type=MESH), c)[1], 0)
    pl.semaphore_wait(barrier, sp - 1 + tp - 1)

    by_core = 1 - lax.rem(t, 2) if B1 == B2 else 1
    down = Gather(p, lambda i, y, x: db.at[i, y, x, td],
                  lambda k: db.at[a, p.y, p.x, td], by_core,
                  (dls, dlr, dfs, dfr, dgs, dgr),
                  (lambda i: db.at[i, :, :, td], dps, dpr) if dtp > 1 else None)
    keys = Gather(p, lambda i, y, x: kb.at[i, y, x, t],
                  lambda k: kb.at[a, p.y, p.x, t], by_core,
                  (kls, klr, kfs, kfr, kgs, kgr),
                  (lambda i: kb.at[i, :, :, t], kps, kpr), causal=True)
    value = Gather(p, lambda i, y, x: vb.at[i, y, x],
                   lambda k: wv.at[:, columns(k)], 1, (vls, vlr, vfs, vfr, vgs, vgr))
    gate = Gather(p, lambda i, y, x: gb.at[i, y, x],
                  lambda k: wg.at[:, columns(k)], 0, (gls, glr, gfs, gfr, ggs, ggr))

    lane = lax.broadcasted_iota(jnp.int32, (R, LANES), 1)
    tok_pair = lambda k: remote(tok, xin.at[:, mine], tsend.at[k - 1], trecv.at[k - 1], p.in_tp(k))
    steps = {}

    def named(f):
        steps[f.__name__] = f
        return f

    @named
    def tok_start():
        each(1, tp, lambda k: tok_pair(k).start())

    @named
    def down_own():
        c_ld.wait()
        c_wr.wait()
        drt[...] = dr[...].astype(f32).T
        db[a, p.y, p.x, td, :, :L] = dl[...]
        db[a, p.y, p.x, td, :, L:] = drt[dpart].astype(bf16)
        down.spread(0)

    for name, g in (("down", down), ("keys", keys), ("value", value), ("gate", gate)):
        steps[name + "_spread"] = lambda g=g: g.spread(0)
        for k in range(A):
            if k:
                steps[f"{name}_line.{k}"] = lambda g=g, k=k: g.start_line(k)
                steps[f"{name}_1.{k}"] = lambda g=g, k=k: g.on_line(k)
            steps[f"{name}_2.{k}"] = lambda g=g, k=k: g.on_first(k)
            steps[f"{name}_3.{k}"] = lambda g=g, k=k: g.on_second(k)
            steps[f"{name}_4.{k}"] = lambda g=g, k=k: g.on_pair(k)

    NR = 32 if R % 32 == 0 else R

    @named
    def norm():
        c_tok.wait()
        each(1, tp, lambda k: tok_pair(k).wait_recv())

        def rows_norm(i, c):
            rows = pl.ds(pl.multiple_of(i * NR, NR), NR)
            v = xin[rows].astype(f32)
            scale = lax.rsqrt(jnp.mean(v * v, axis=-1, keepdims=True) + epsilon)
            xb[a, rows] = (v * scale * gain[...]).astype(bf16)
            return c
        lax.fori_loop(0, R // NR, rows_norm, 0)

    @named
    def rope_own():
        c0, s0 = far[0, pl.ds(s, 1)], far[1, pl.ds(s, 1)]
        cosine[...] = near[0] * c0 - near[1] * s0
        sine[...] = near[1] * c0 + near[0] * s0

    def hop(way, j):
        i = jnp.clip(a + (-j if way == 0 else j), 0, A - 1)
        to = jnp.clip(a + (1 if way == 0 else -1), 0, A - 1)
        return remote(xb.at[i, :, mine], xb.at[i, :, mine], zsend.at[way, j],
                      zrecv.at[way, j], p.at(to, p.y, p.x))

    def across(way, j, k):
        i = jnp.clip(a + (2 * way - 1) * j, 0, A - 1)
        return remote(xb.at[i, :, mine], xb.at[i, :, mine], psend.at[way, j - 1, k - 1],
                      precv.at[way, j - 1, k - 1], p.in_tp(k))

    def has(way, j):
        return a - j >= 0 if way == 0 else a + j < A

    def onward(way):
        return a + 1 < A if way == 0 else a >= 1

    def start_hop(way, j):
        if j < A - 1:
            pl.when(jnp.logical_and(has(way, j), onward(way)))(lambda: hop(way, j).start())

    def token_step(j):
        for way in (0, 1):
            def got(way=way):
                hop(way, j - 1).wait_recv()
                each(1, tp, lambda k: across(way, j, k).start())
            pl.when(has(way, j))(got)
            start_hop(way, j)

    @named
    def tok_0():
        start_hop(0, 0)
        start_hop(1, 0)

    for j in range(1, A):
        steps[f"tok_{j}"] = lambda j=j: token_step(j)

    @named
    def query_0():
        c_kup.wait()

    def query(i):
        c_wq[i].wait()
        q = dot(xb[a], wqb[:, i * step:(i + 1) * step]).astype(bf16).astype(f32)
        q0, q1, q2 = q[:, :LANES], q[:, LANES:2 * LANES], q[:, 2 * LANES:]
        left = lane < ROPE
        second = jnp.where(left, pltpu.roll(q1, ROPE, 1), pltpu.roll(q2, ROPE, 1))
        ropes = jnp.where(left, q1, q2)
        turned = ropes * cosine[...] + swap_halves(ropes, lane) * sine[...]
        for h, plain, rope in ((0, q0, turned), (1, second, pltpu.roll(turned, ROPE, 1))):
            at = 2 * i + h
            up = kupb[:, at * PLAIN:(at + 1) * PLAIN]
            rows = pl.ds(at * R, R)
            qs[:L, rows] = dot_nt(up, plain.astype(bf16)).astype(bf16)
            qs[L:, rows] = rope.T[:ROPE].astype(bf16)

    for i in range(4):
        steps[f"query_{i + 1}"] = lambda i=i: each(
            i, heads // 2 if i == 3 else min(i + 1, heads // 2), query)

    @named
    def keys_own():
        own = xb[a, pl.ds(pl.multiple_of(t * Rk, Rk), Rk)]
        span = D // A
        pre = jnp.zeros((Rk, E), f32)
        for i in range(A):
            pre = pre + dot(own[:, i * span:(i + 1) * span], db[i].reshape(span, E))
        lat = pre[:, :L]
        lat = lat * lax.rsqrt(
            jnp.mean(lat * lat, axis=-1, keepdims=True) + epsilon) * lgain[...]
        rope = jnp.concatenate([pre[:, L:], pre[:, L:]], axis=1)
        krows = pl.ds(pl.multiple_of(t * Rk, Rk), Rk)
        rope = rope * cosine[krows] + swap_halves(rope, lane[:Rk]) * sine[krows]
        kb[a, p.y, p.x, t, :, :L] = lat.astype(bf16)
        kb[a, p.y, p.x, t, :, L:] = rope[:, :ROPE].astype(bf16)

    per = 1
    while per < B2 and (per * 2) * R <= 512 and B2 % (per * 2) == 0:
        per *= 2
    tall = 1
    if per == B2:
        while tall < B1 and (tall * 2) * per * R <= 512 and B1 % (tall * 2) == 0:
            tall *= 2
    KS = tall * per * R
    QR = ROWS if heads * R % ROWS == 0 else R
    blocks = heads * R // QR
    unroll = UNROLL if blocks % UNROLL == 0 else 1
    grade = HEAD ** (-0.5) * 1.4426950408889634

    def each_row(body):
        def some(i, c):
            for u in range(unroll):
                body(i * unroll + u)
            return c
        if blocks == unroll:
            some(0, 0)
        else:
            lax.fori_loop(0, blocks // unroll, some, 0)

    @named
    def attend_init():
        mx[...] = jnp.full(mx.shape, masked_score, f32)
        sm[...] = jnp.zeros(sm.shape, f32)
        acc[...] = jnp.zeros(acc.shape, f32)

    def attend(i, k0, kk, kt, masked):
        rows = pl.ds(pl.multiple_of(i * QR, QR), QR)
        sc = dot(kk, qs[:, rows])
        if masked:
            kp = lax.broadcasted_iota(jnp.int32, (KS, QR), 0)
            at = lax.broadcasted_iota(jnp.int32, (KS, QR), 1)
            allowed = kp - lax.rem(at, R) <= s * R - k0
            sc = jnp.where(allowed, sc, masked_score)
        old = mx[:, rows]
        new = jnp.maximum(old, jnp.max(sc, axis=0, keepdims=True))
        w = jnp.exp2((sc - new) * grade)
        fade = jnp.exp2((old - new) * grade)
        sm[:, rows] = fade * sm[:, rows] + jnp.sum(w, axis=0, keepdims=True)
        mx[:, rows] = new
        acc[:, rows] = fade * acc[:, rows] + dot(kt, w.astype(bf16))

    def chunk(k):
        def go():
            c = p.back(k)

            def sub(n):
                y0 = n // (B2 // per) * tall
                x0 = lax.rem(n, B2 // per) * per
                kk = kb[c, pl.ds(y0, tall), pl.ds(x0, per)].reshape(KS, E)
                k0 = (c * B + y0 * B2 + x0) * R
                kt = kk[:, :L].T
                each_row(lambda i: attend(i, k0, kk, kt, k == 0))
            if B * R == KS:
                sub(0)
            else:
                def maybe(n, q):
                    pl.when(c * B + n * (KS // R) <= s)(lambda: sub(n))
                    return q
                lax.fori_loop(0, B * R // KS, maybe, 0)
        pl.when(k <= a)(go)

    for k in range(A):
        steps[f"attend_{k}"] = lambda k=k: chunk(k)
    NT = 512
    nt = D // NT

    @named
    def attend_out():
        c_vup.wait()
        c_wma.wait()
        for h in range(heads):
            rows = pl.ds(h * R, R)
            out = (acc[:, rows] / sm[:, rows]).T.astype(bf16)
            att[:, h * VALUE:(h + 1) * VALUE] = dot(
                out, vupb[:, h * VALUE:(h + 1) * VALUE]).astype(bf16)
            logs[h:h + 1] = mx[:, rows] * HEAD ** (-0.5) + jnp.log(sm[:, rows])

        def attn_merge(n, c):
            cols = pl.ds(pl.multiple_of(n * NT, NT), NT)
            pacc[:, cols] = dot(att[...], wmab[:, cols])
            return c
        lax.fori_loop(0, nt, attn_merge, 0)

    def block(way, j):
        return jnp.clip(a + (2 * way - 1) * j, 0, A - 1)

    def there(place, way, j):
        i = place + (2 * way - 1) * j
        return jnp.logical_and(i >= 0, i < A)

    swap = lambda way, j: remote(
        gated.at[block(way, j)], cb.at[a, pl.ds(HALO, R)], wsend.at[way, j - 1],
        wrecv.at[way, j - 1], p.at(block(way, j), p.y, p.x))

    def after(i):
        return i * B + p.b + 1

    def halo(way, j):
        i = block(way, j)
        to = jnp.minimum(after(i), sp - 1)
        return remote(gated.at[i, pl.ds(R - HALO, HALO)], cb.at[a, pl.ds(0, HALO)],
                      hsend.at[way, j], hrecv.at[way, j], {"sp": to, "tp": t})

    def project(i):
        rows = xb[i]
        v = dot(rows, vb[...].reshape(D, W))
        g = dot(rows, gb[...].reshape(D, W))
        gated[i] = (v / (1.0 + jnp.exp(-g))).astype(bf16)

    def gated_at(j):
        def side(way, c):
            def go():
                each(1, tp, lambda k: across(way, j, k).wait_recv())
                project(block(way, j))
                swap(way, j).start()
                pl.when(after(block(way, j)) < sp)(lambda: halo(way, j).start())
            pl.when(there(a, way, j))(go)
            return c
        lax.fori_loop(0, 2, side, 0)

    for j in range(1, A):
        steps[f"gated_{j}"] = lambda j=j: gated_at(j)

    @named
    def wready():
        c_v.wait()
        c_g.wait()

    @named
    def gated_0():
        project(a)
        cb[a, HALO:] = gated[a]
        pl.when(after(a) < sp)(lambda: halo(0, 0).start())
        pl.when(s == 0)(lambda: cb.__setitem__(
            (slice(None), slice(0, HALO)), jnp.zeros((A, HALO, W), bf16)))

    both_ways = [(way, j) for j in range(1, A) for way in (0, 1)]

    def halos():
        from_line = (s - 1) // B
        halo(0, 0).wait_recv()
        for way, j in both_ways:
            pl.when(there(from_line, 1 - way, j))(
                lambda way=way, j=j: halo(way, j).wait_recv())

    reach = taps.shape[0] - 1
    lead = HALO - reach
    whole = R + HALO
    wb = W // LANES

    def convolve(n, c):
        i = n // wb
        cols = pl.ds(pl.multiple_of(lax.rem(n, wb) * LANES, LANES), LANES)
        full = pl.ds(pl.multiple_of(n * LANES, LANES), LANES)
        xf = cb[i, :, cols].astype(f32)
        tw = taps[:, full].astype(f32)
        out = jnp.zeros((R, LANES), f32)
        for r in range(8):
            xr = xf if r == 0 else pltpu.roll(xf, whole - r, 0)
            for m in range(HALO // 8 + 1):
                j = 8 * m + r - lead
                if 0 <= j <= reach:
                    out = out + tw[j:j + 1] * xr[8 * m:8 * m + R]
        mixed[:, full] = out
        return c

    stats = lambda k: remote(st.at[t], st.at[t], ssend.at[k - 1], srecv.at[k - 1], p.in_tp(k))

    @named
    def conv():
        pl.when(s > 0)(halos)
        for way, j in both_ways:
            pl.when(there(a, 1 - way, j))(lambda way=way, j=j: swap(way, j).wait_recv())
        lax.fori_loop(0, A * wb, convolve, 0)
        all_mixed = mixed[...]
        one = jnp.sum(all_mixed, axis=1, keepdims=True)
        two = jnp.sum(all_mixed * all_mixed, axis=1, keepdims=True)
        st[t] = jnp.where(lane == 0, one, jnp.where(lane == 1, two, 0.0))
        each(1, tp, lambda k: stats(k).start())

    share = lambda n, k: remote(
        pb.at[lax.rem(t + k, tp), :, pl.ds(n * NT, NT)], hold.at[t, :, pl.ds(n * NT, NT)],
        msend.at[n, k - 1], mrecv.at[n, k - 1], p.in_tp(k))

    @named
    def finish():
        each(1, tp, lambda k: stats(k).wait_recv())
        both = jnp.sum(st[...], axis=0)
        mean = both[:, :1] / (C * tp)
        var = both[:, 1:2] / (C * tp) - mean * mean
        z = (mixed[...] - mean) * lax.rsqrt(var + epsilon) * cgain[...]
        out = (z / (1.0 + jnp.exp(-z))).astype(bf16)
        c_wmc.wait()
        for n in range(nt):
            cols = slice(n * NT, (n + 1) * NT)
            part = (dot(out, wmcb[:, cols]) + pacc[:, cols]).astype(bf16)
            for j in range(tp):
                pb[j, :, cols] = part[j * Rk:(j + 1) * Rk]
            each(1, tp, lambda k: share(n, k).start())

    for name in ORDER:
        if name in steps:
            steps[name]()
    hold[t] = pb[t]

    each(1, tp, lambda k: tok_pair(k).wait_send())
    for g in (down, keys, value, gate):
        g.drain()
    for way in (0, 1):
        for j in range(A - 1):
            pl.when(jnp.logical_and(has(way, j), onward(way)))(
                lambda way=way, j=j: hop(way, j).wait_send())
        for j in range(1, A):
            pl.when(has(way, j))(lambda way=way, j=j: each(
                1, tp, lambda k: across(way, j, k).wait_send()))
    for way, j in both_ways:
        def sent(way=way, j=j):
            swap(way, j).wait_send()
            pl.when(after(block(way, j)) < sp)(lambda: halo(way, j).wait_send())
        pl.when(there(a, way, j))(sent)
    pl.when(after(a) < sp)(lambda: halo(0, 0).wait_send())
    each(1, tp, lambda k: stats(k).wait_send())
    for n in range(nt):
        each(1, tp, lambda k: share(n, k).wait())


def total_kernel(hold, logs, merged, log_sums):
    whole_sum = hold[0].astype(f32)
    for j in range(1, hold.shape[0]):
        whole_sum = whole_sum + hold[j].astype(f32)
    merged[...] = whole_sum.astype(bf16)
    log_sums[...] = logs[...]


def rope_tables(positions):
    lanes = np.arange(LANES)
    inverse = rope_base ** (-2.0 * (lanes % (ROPE // 2)) / ROPE)
    sign = np.where(lanes % ROPE < ROPE // 2, -1.0, 1.0)
    angle = np.asarray(positions, np.float64)[:, None] * inverse[None, :]
    return jnp.asarray(np.stack([np.cos(angle), np.sin(angle) * sign]), f32)


def local(tokens, norm_gain, w_value, w_gate, conv_taps, conv_gain, w_query,
          latent_down_weight, latent_norm_gain, w_rope_key, key_up_weight,
          value_up_weight, w_merge_conv, w_merge_attn):
    R, F = tokens.shape
    sp, tp = lax.axis_size("sp"), lax.axis_size("tp")
    C = w_value.shape[1]
    A = 1
    while A < 4 and sp % (2 * A) == 0 and C % (2 * A * LANES) == 0:
        A *= 2
    B = sp // A
    B2 = 1
    while B2 * B2 < B and B % (2 * B2) == 0:
        B2 *= 2
    B1 = B // B2
    D = w_query.shape[0]
    L = latent_down_weight.shape[1]
    E = L + ROPE
    W = C // A
    Kr = w_value.shape[0]
    heads = w_query.shape[1] // HEAD
    Rk = R // tp
    dtp = tp if Kr % (16 * tp) == 0 else 1
    NT = D // 512
    S = pltpu.SemaphoreType.DMA
    V = pltpu.VMEM
    two = lambda *n: [S(n), S(n)]
    most = max(B1, B2)
    gather = lambda F, G: two(A - 1) + two(A, F - 1) + two(A, F, G - 1)
    by_core = (most, most) if B1 == B2 else (B2, B1)
    sds = jax.ShapeDtypeStruct
    row = lambda v: v.reshape(1, -1)
    hold, logs = pl.pallas_call(
        lambda *refs: kernel(A, B1, B2, tp, dtp, *refs),
        out_shape=(V((tp, Rk, D), bf16), V((heads, R), f32)),
        in_specs=[ANY] * 10 + [VMEM] * 6,
        out_specs=(VMEM, VMEM),
        scratch_shapes=[
            V((R, LANES), f32), V((R, LANES), f32), V((R, D), bf16), V((A, R, D), bf16),
            V((A, B1, B2, Kr, W), bf16), V((A, B1, B2, Kr, W), bf16),
            V((A, B1, B2, dtp, Kr // dtp, E), bf16), V((A, B1, B2, tp, Rk, E), bf16),
            V((Kr // dtp, L), bf16), V((ROPE, Kr), bf16), V((Kr, ROPE), f32),
            V(w_query.shape, bf16), V(key_up_weight.shape, bf16),
            V(value_up_weight.shape, bf16), V(w_merge_conv.shape, bf16),
            V(w_merge_attn.shape, bf16),
            V((E, heads * R), bf16), V((L, heads * R), f32),
            V((1, heads * R), f32), V((1, heads * R), f32),
            V((R, heads * VALUE), bf16), V((R, D), f32),
            V((A, R, W), bf16), V((A, R + HALO, W), bf16), V((R, C), f32),
            V((tp, R, LANES), f32), V((tp, Rk, D), bf16),
            S((10 + heads // 2,)), *two(tp - 1), *two(2, A - 1), *two(2, A - 1, tp - 1),
            *gather(*by_core), *two(A, tp - 1), *gather(*by_core), *two(A, tp - 1),
            *gather(B2, B1), *gather(B1, B2),
            *two(2, A - 1), *two(2, A), *two(tp - 1), *two(NT, tp - 1),
        ],
        compiler_params=pltpu.CompilerParams(
            collective_id=0, has_side_effects=True, vmem_limit_bytes=60 * 2**20),
        name="layer",
    )(*(pltpu.with_memory_space_constraint(v, pltpu.HBM) for v in (
        tokens, w_value, w_gate, w_query, latent_down_weight, w_rope_key.T, key_up_weight,
        value_up_weight, w_merge_conv, w_merge_attn)), row(norm_gain), row(latent_norm_gain),
      row(conv_gain), conv_taps, rope_tables(range(R)), rope_tables(range(0, sp * R, R)))
    merged, logs = pl.pallas_call(
        total_kernel,
        out_shape=(sds((Rk, D), bf16), sds((heads, R), f32)),
        in_specs=[VMEM] * 2,
        out_specs=(VMEM,) * 2,
        compiler_params=pltpu.CompilerParams(vmem_limit_bytes=4 * 2**20),
        name="total",
    )(hold, logs)
    return merged, logs.T


def solution(mesh):
    return jax.shard_map(
        local,
        mesh=mesh,
        in_specs=(
            P("sp", "tp"), P(), P("sp", "tp"), P("sp", "tp"), P(None, "tp"), P("tp"),
            P(None, "tp"), P("sp", None), P(), P("sp", None), P(None, "tp"),
            P(None, "tp"), P("tp", None), P("tp", None),
        ),
        out_specs=(P(("sp", "tp"), None), P("sp", "tp")),
        check_vma=False,
    )
```
